256 devices in a mesh: sp: 32 (over z, y), dp: 8 (over x, core).
Axes of the slice: x: 4, y: 4, z: 8, core: 2. Of those that a mesh axis runs over, the one named last changes fastest.
Arguments:
- queries: bfloat16 [8, 2048, 5120], P('dp', None, 'sp'), may hold values from -6 to 6
- keys: bfloat16 [8, 1024, 5120], P('dp', None, 'sp'), may hold values from -6 to 6
- values: bfloat16 [8, 1024, 5120], P('dp', None, 'sp'), may hold values from -48 to 48
- q_gain: float32 [64], replicated, may hold values from 0.5 to 10
- k_gain: float32 [64], replicated, may hold values from 0.5 to 10
- w_out: bfloat16 [2048, 2048], P(None, 'dp'), may hold values from -0.125 to 0.125
Outputs:
- mixed: bfloat16 [8, 5120, 2048], P('dp', 'sp')
The draws below stay inside these ranges and needn't reach their ends.
All inputs are finite; a program needn't handle non-finite values.
Results may differ from the reference program's by a relative error of at most 0.0038.
The reference program's roundings to bfloat16 on the way count: a program that leaves them out, or rounds other values in their place, can miss the bound.
Values may be sent and summed in bfloat16 or wider, within the bound.
A program may use at most 64 MiB of HBM per device.

```python
import jax
import jax.numpy as jnp
from jax import lax

HD = 64
QH = 32
KV = 16
D = 2048
GRID_W = 64
QW = 2048
KVW = 1024
TOKENS = 5120
SEQ_GROUPS = 8


def shared_keys(key):
    key_draw = jax.random.normal(jax.random.fold_in(key, 11), (SEQ_GROUPS, KVW, TOKENS), jnp.float32)
    return jnp.clip(key_draw, -6.0, 6.0)


def draw_keys(key, part):
    return shared_keys(key).astype(jnp.bfloat16)


def draw_queries(key, part):
    fresh_draw = jax.random.normal(jax.random.fold_in(key, 12), (SEQ_GROUPS, QW, TOKENS), jnp.float32)
    fresh_draw = jnp.clip(fresh_draw, -6.0, 6.0)
    return fresh_draw.astype(jnp.bfloat16)


def gain_draw(key, salt):
    noise_draw = jnp.clip(jax.random.normal(jax.random.fold_in(key, salt), (HD,), jnp.float32), -3.0, 3.0)
    return 1.25 * (1.0 + 0.18 * noise_draw)


def draw_q_gain(key, part):
    return gain_draw(key, 21)


def draw_k_gain(key, part):
    return gain_draw(key, 22)


def steps_of(rng, dims, split, least, top_value):
    level = 1.0
    for axis_at, parts in split:
        draws = jax.random.uniform(jax.random.fold_in(jax.random.fold_in(rng, 6), axis_at), (parts,), jnp.float32, least / len(split), top_value / len(split))
        level = level * jnp.repeat(jnp.exp(draws), dims[axis_at] // parts).reshape((-1,) + (1,) * (len(dims) - 1 - axis_at))
    return level


def noise(rng, shape, spread, reach, split=(), held_as=jnp.bfloat16):
    result = jax.random.normal(rng, shape, jnp.float32) * spread
    if len(split) > 0:
        result = steps_of(rng, shape, split, -0.22, 0.18) * result
    return jnp.clip(result, min=-reach, max=reach).astype(held_as)


def setup_inputs(seed: int = 0) -> dict:
    key_list = jax.random.split(jax.random.key(seed), 7)
    queries = draw_queries(jax.random.fold_in(key_list[6], 71), 0)
    keys = draw_keys(jax.random.fold_in(key_list[6], 71), 0)
    values = noise(key_list[2], (SEQ_GROUPS, KVW, TOKENS), 8.0, 48.0, ((0, 8), (2, 32)))
    q_gain = draw_q_gain(jax.random.fold_in(key_list[6], 71), 0)
    k_gain = draw_k_gain(jax.random.fold_in(key_list[6], 71), 0)
    w_out = noise(key_list[5], (QW, D), QW ** -0.5, 0.125, ((1, 8),))
    return dict(queries=queries, keys=keys, values=values, q_gain=q_gain, k_gain=k_gain, w_out=w_out)


epsilon = 1e-06
rotary_base = 10000.0

def rotary_tables(row_count):
    position = jnp.arange(row_count, dtype=jnp.int32)
    grid_row = (position // GRID_W).astype(jnp.float32)
    grid_col = (position % GRID_W).astype(jnp.float32)
    quarter = HD // 4
    inv_freq = rotary_base ** (-(2.0 * jnp.arange(quarter, dtype=jnp.float32)) / (HD // 2))
    row_angle = inv_freq[:, None] * grid_row[None, :]
    col_angle = inv_freq[:, None] * grid_col[None, :]
    cos_table = jnp.concatenate([jnp.cos(row_angle), jnp.cos(row_angle), jnp.cos(col_angle), jnp.cos(col_angle)], axis=0)
    sin_table = jnp.concatenate([jnp.sin(row_angle), jnp.sin(row_angle), jnp.sin(col_angle), jnp.sin(col_angle)], axis=0)
    return (cos_table, sin_table)

def normalize_turn(field, gain, cos_table, sin_table):
    head_count = field.shape[0] // HD
    values_f = field.astype(jnp.float32).reshape(head_count, HD, field.shape[1])
    normed = values_f * lax.rsqrt(lax.optimization_barrier(jnp.mean(values_f * values_f, axis=1, keepdims=True)) + epsilon) * gain[None, :, None]
    quarter = HD // 4
    quarters_of = normed.reshape(head_count, 4, quarter, field.shape[1])
    turned = jnp.concatenate([-quarters_of[:, 1], quarters_of[:, 0], -quarters_of[:, 3], quarters_of[:, 2]], axis=1)
    return (normed * cos_table[None] + turned * sin_table[None]).astype(jnp.bfloat16)

def reference(queries, keys, values, q_gain, k_gain, w_out):
    cos_table, sin_table = rotary_tables(TOKENS)
    group_size = QH // KV
    score_scale = HD ** (-0.5)

    def per_group(packed):
        query_rows, key_rows, value_rows = packed
        query_rot = normalize_turn(query_rows, q_gain, cos_table, sin_table)
        key_rot = normalize_turn(key_rows, k_gain, cos_table, sin_table)
        value_heads = value_rows.reshape(KV, HD, TOKENS)

        def per_head(head_index):
            query_one = lax.dynamic_index_in_dim(query_rot, head_index, 0, keepdims=False)
            key_one = lax.dynamic_index_in_dim(key_rot, head_index // group_size, 0, keepdims=False)
            value_one = lax.dynamic_index_in_dim(value_heads, head_index // group_size, 0, keepdims=False)
            scores = jnp.einsum('dq,dk->qk', query_one.astype(jnp.float32), key_one.astype(jnp.float32)) * score_scale
            row_max = lax.optimization_barrier(jnp.max(scores, axis=-1, keepdims=True))
            weights = jnp.exp(scores - row_max)
            weights = (weights / lax.optimization_barrier(jnp.sum(weights, axis=-1, keepdims=True))).astype(jnp.bfloat16)
            attended = jnp.einsum('qk,dk->dq', weights.astype(jnp.float32), value_one.astype(jnp.float32))
            return attended.astype(jnp.bfloat16)
        attended = lax.map(per_head, jnp.arange(QH, dtype=jnp.int32)).reshape(QW, TOKENS)
        return jnp.dot(attended.T, w_out, preferred_element_type=jnp.float32).astype(jnp.bfloat16)
    return lax.map(per_group, (queries, keys, values))
```

```python
import jax
import jax.numpy as jnp
from jax import lax
from jax.experimental import pallas as pl
from jax.experimental.pallas import tpu as pltpu
from jax.sharding import PartitionSpec as P

HD = 64
QH = 32
KV = 16
GRID_W = 64
Z = 8
Y = 4
X = 4
TOK = 160
KEYS = 5120
TQ = 256
TILES = 20
KC = 256
GROUP = 4
SPAN = GROUP * TOK
W_ROWS = 2048
W_COLS = 256

epsilon = 1e-06
rotary_base = 10000.0
log2_scale = HD ** (-0.5) * 1.4426950408889634
f32 = jnp.float32
bf16 = jnp.bfloat16
MESH = pl.DeviceIdType.MESH


def rotary_tables(first_row, row_count):
    position = first_row + lax.iota(jnp.int32, row_count)
    grid_row = (position // GRID_W).astype(f32)
    grid_col = (position % GRID_W).astype(f32)
    quarter = HD // 4
    inv_freq = rotary_base ** (-(2.0 * lax.iota(f32, quarter)) / (HD // 2))
    row_angle = inv_freq[:, None] * grid_row[None, :]
    col_angle = inv_freq[:, None] * grid_col[None, :]
    cos_table = jnp.concatenate(
        [jnp.cos(row_angle), jnp.cos(row_angle), jnp.cos(col_angle), jnp.cos(col_angle)], axis=0
    )
    sin_table = jnp.concatenate(
        [jnp.sin(row_angle), jnp.sin(row_angle), jnp.sin(col_angle), jnp.sin(col_angle)], axis=0
    )
    return (cos_table, sin_table)


def turned(field, gain, cos_table, sin_table):
    u = field.astype(f32)
    n = u * lax.rsqrt(jnp.mean(u * u, axis=0, keepdims=True) + epsilon) * gain
    rot = jnp.concatenate([-n[16:32], n[0:16], -n[48:64], n[32:48]], axis=0)
    return n * cos_table + rot * sin_table


class Place:
    def __init__(self):
        sp = lax.axis_index("sp")
        self.dp = lax.axis_index("dp")
        self.z, self.y = lax.div(sp, Y), lax.rem(sp, Y)
        self.g = lax.div(self.y, 2)
        self.e = self.g * (3 - self.y) + (1 - self.g) * self.y
        self.head = 2 * self.z + self.e
        self.partner = self.z * Y + 3 - self.y
        x, self.c = lax.div(self.dp, 2), lax.rem(self.dp, 2)
        self.left = lax.rem(x + X - 1, X) * 2 + self.c
        self.right = lax.rem(x + 1, X) * 2 + self.c
        self.sib = self.dp + 1 - 2 * self.c
        self.opp = lax.rem(x + 2, X) * 2 + self.c

    def offset(self, n):
        i = lax.div(n, 2)
        return lax.div(i + 1, 2) * (2 * lax.rem(i, 2) - 1)

    def at(self, z, e):
        return z * Y + self.g * 3 + e * (1 - 2 * self.g)

    def target_z(self, n):
        return lax.rem(self.z + self.offset(n) + Z, Z)

    def source_z(self, n):
        return lax.rem(self.z - self.offset(n) + Z, Z)

    def slot_there(self, n):
        return 2 * lax.div(n, 2) + self.e


def loop(count, body):
    def step(n, carry):
        body(n)
        return carry

    lax.fori_loop(0, count, step, 0)


def attention_step(q, top, scale, kk, vt, x_ref, y_ref, scores=True, exps=True, sums=True):
    m = jnp.full((8, TQ), -jnp.inf, f32)
    total = jnp.zeros((8, TQ), f32)
    out = None
    for j in range(KEYS // KC):
        at = slice(j * KC, (j + 1) * KC)
        if sums:
            weights = (x_ref[at, :] * scale).astype(bf16)
            part = lax.dot_general(
                vt[:, at], weights, (((1,), (0,)), ((), ())), preferred_element_type=f32
            )
            out = part if out is None else out + part
        if scores:
            k = kk[at, :]
            s = lax.dot_general(
                jnp.concatenate([k, k], axis=1), q, (((1,), (0,)), ((), ())), preferred_element_type=f32
            )
            x_ref[at, :] = s
            m = jnp.maximum(m, jnp.max(s.reshape(KC // 8, 8, TQ), axis=0))
        if exps:
            e = jnp.exp2(y_ref[at, :] - top)
            y_ref[at, :] = e
            total = total + jnp.sum(e.reshape(KC // 8, 8, TQ), axis=0)
    return m, total, out


def layer(
    q_ref, k_ref, v_ref, w_ref, cos_ref, sin_ref, qg_ref, kg_ref, out_ref,
    kvs, qs, kvr, qr, kk, vt, qt, s0, s1, ot, atts, attr, wf,
    kv_ss, kv_rs, fw_ss, fw_rs, q_ss, q_rs, at_ss, at_rs, w_ss, w_rs, own_sem,
):
    me = Place()

    def remote(src, dst, ss, rs, **device):
        return pltpu.make_async_remote_copy(
            src_ref=src, dst_ref=dst, send_sem=ss, recv_sem=rs, device_id=device, device_id_type=MESH
        )

    barrier = pltpu.get_barrier_semaphore()

    def hello(**device):
        pl.semaphore_signal(barrier, inc=1, device_id=device, device_id_type=MESH)

    def greet(n):
        @pl.when(n != me.e)
        def _():
            hello(sp=me.at(me.target_z(n), lax.rem(n, 2)))

    loop(16, greet)
    hello(sp=me.partner)
    hello(dp=me.sib)
    hello(dp=me.left)
    hello(dp=me.right)

    cos_table, sin_table = cos_ref[...], sin_ref[...]

    def make_kv(n):
        j = 2 * me.target_z(n) + lax.rem(n, 2)
        rows = pl.ds(pl.multiple_of(j * HD, HD), HD)
        k = turned(k_ref[0, rows, :], kg_ref[...], cos_table, sin_table)
        both = jnp.concatenate([k, v_ref[0, rows, :].astype(f32)], axis=0)
        kvs[n] = jnp.transpose(both).astype(bf16)

    def make_q(n):
        j = 2 * me.target_z(n) + lax.rem(n, 2)
        a = q_ref[0, pl.ds(pl.multiple_of(j * 2 * HD, HD), HD), :]
        b = q_ref[0, pl.ds(pl.multiple_of(j * 2 * HD + HD, HD), HD), :]
        both = jnp.concatenate(
            [turned(a, qg_ref[...], cos_table, sin_table), turned(b, qg_ref[...], cos_table, sin_table)],
            axis=0,
        )
        qs[n] = jnp.transpose(both).astype(bf16)

    def kv_copy(n):
        there = me.slot_there(n)
        return remote(
            kvs.at[n], kvr.at[0, there], kv_ss.at[n], kv_rs.at[there],
            sp=me.at(me.target_z(n), lax.rem(n, 2)),
        )

    def q_copy(n):
        there = me.slot_there(n)
        return remote(
            qs.at[n], qr.at[there], q_ss.at[n], q_rs.at[there],
            sp=me.at(me.target_z(n), lax.rem(n, 2)),
        )

    def fw_copy(n):
        return remote(kvr.at[0, n], kvr.at[1, n], fw_ss.at[n], fw_rs.at[n], sp=me.partner)

    def at_copy(n):
        return remote(
            atts.at[n], attr.at[me.head], at_ss.at[n], at_rs.at[me.head],
            sp=me.at(me.source_z(n), lax.rem(n, 2)),
        )

    def arrival(ref, ss, rs):
        return remote(ref, ref, ss, rs, sp=me.partner)

    top_half, low_half = pl.ds(0, W_ROWS // 2), pl.ds(W_ROWS // 2, W_ROWS // 2)

    def w_copy(kind, src, dst, dp):
        return remote(src, dst, w_ss.at[kind], w_rs.at[kind], dp=dp)

    w_own = (
        w_copy(0, w_ref, wf.at[me.dp], me.sib),
        w_copy(1, w_ref, wf.at[me.dp], me.right),
        w_copy(2, w_ref, wf.at[me.dp], me.left),
    )
    w_next = (
        w_copy(3, wf.at[me.left, top_half], wf.at[me.left, top_half], me.right),
        w_copy(4, wf.at[me.right, low_half], wf.at[me.right, low_half], me.left),
        w_copy(5, wf.at[me.left], wf.at[me.left], me.sib),
        w_copy(6, wf.at[me.right], wf.at[me.right], me.sib),
    )
    w_last = (
        w_copy(7, wf.at[me.opp, top_half], wf.at[me.opp, top_half], me.sib),
        w_copy(8, wf.at[me.opp, low_half], wf.at[me.opp, low_half], me.sib),
    )

    def w_arrival(kind, ref):
        arrival(ref, w_ss.at[kind], w_rs.at[kind]).wait_recv()

    loop(16, make_kv)
    pl.semaphore_wait(barrier, 19)

    def send_kv(n):
        @pl.when(n != me.e)
        def _():
            kv_copy(n).start()

        make_q(n)

    loop(16, send_kv)

    def send_q(n):
        @pl.when(n != me.e)
        def _():
            q_copy(n).start()

    loop(16, send_q)
    own_w = pltpu.make_async_copy(w_ref, wf.at[me.dp], own_sem)
    own_w.start()
    for copy in w_own:
        copy.start()
    kvr[0, me.e] = kvs[me.e]
    qr[me.e] = qs[me.e]

    def forward(n):
        @pl.when(n != me.e)
        def _():
            arrival(kvr.at[0, n], kv_ss.at[n], kv_rs.at[n]).wait_recv()

        fw_copy(n).start()

    loop(16, forward)

    def make_keys(half, g):
        block = kvr[half, pl.ds(GROUP * g, GROUP)].reshape(SPAN, 2 * HD)
        at = pl.ds(pl.multiple_of((half * GROUP + g) * SPAN, 128), SPAN)
        kk[at, :] = jnp.concatenate([block[:, :HD], block[:, :HD]], axis=1)
        vt[:, at] = jnp.transpose(block)[HD:]

    loop(4, lambda g: make_keys(0, g))

    def partner_keys(g):
        def wait(n):
            arrival(kvr.at[1, GROUP * g + n], fw_ss.at[GROUP * g + n], fw_rs.at[GROUP * g + n]).wait_recv()

        loop(4, wait)
        make_keys(1, g)

    loop(4, partner_keys)

    def make_queries(g):
        def wait(r):
            n = GROUP * g + r

            @pl.when(n != me.e)
            def _():
                arrival(qr.at[n], q_ss.at[n], q_rs.at[n]).wait_recv()

        loop(4, wait)
        block = qr[pl.ds(GROUP * g, GROUP)].reshape(SPAN, 2 * HD)
        t = jnp.transpose(block.astype(f32)) * log2_scale
        t = jnp.concatenate([t[:HD], t[HD:]], axis=1)
        first = t.astype(bf16)
        rest = t - first.astype(f32)
        second = rest.astype(bf16)
        third = (rest - second.astype(f32)).astype(bf16)
        terms = jnp.concatenate([first, second, third, jnp.zeros_like(third)], axis=0)
        for u in range(5):
            qt[5 * g + u] = terms[:, u * TQ : (u + 1) * TQ]

    def send_back(g):
        tiles = jnp.concatenate([ot[5 * g + u] for u in range(5)], axis=1)
        heads = jnp.concatenate([tiles[:, :SPAN], tiles[:, SPAN:]], axis=0)
        atts[pl.ds(GROUP * g, GROUP)] = jnp.transpose(heads).astype(bf16).reshape(GROUP, TOK, 2 * HD)

        def send(r):
            n = GROUP * g + r

            @pl.when(n != me.e)
            def _():
                at_copy(n).start()

        loop(4, send)

    make_queries(0)
    row_top = lambda m: jnp.max(m, axis=0, keepdims=True)
    row_scale = lambda total: 1.0 / jnp.sum(total, axis=0, keepdims=True)
    s1[...] = jnp.zeros_like(s1)
    m, _, _ = attention_step(qt[0], None, None, kk, vt, s0, None, exps=False, sums=False)

    def two_tiles(p, carry):
        top, scale = carry

        @pl.when(jnp.logical_or(p == 2, jnp.logical_or(p == 4, p == 7)))
        def _():
            make_queries(lax.div(p, 2))

        @pl.when(p == 3)
        def _():
            w_arrival(1, wf.at[me.left])
            w_arrival(2, wf.at[me.right])
            for copy in w_next:
                copy.start()

        @pl.when(p == 8)
        def _():
            w_arrival(3, wf.at[me.opp, top_half])
            w_arrival(4, wf.at[me.opp, low_half])
            for copy in w_last:
                copy.start()

        m, total, out = attention_step(qt[2 * p + 1], top, scale, kk, vt, s1, s0)
        ot[jnp.maximum(2 * p - 1, 0)] = out
        top, scale = row_top(m), row_scale(total)
        m, total, out = attention_step(
            qt[jnp.minimum(2 * p + 2, TILES - 1)], top, scale, kk, vt, s0, s1
        )
        ot[2 * p] = out

        @pl.when(jnp.logical_or(p == 2, jnp.logical_or(p == 5, p == 7)))
        def _():
            send_back(lax.div(p, 3))

        return row_top(m), row_scale(total)

    _, scale = lax.fori_loop(
        0, TILES // 2, two_tiles, (row_top(m), jnp.zeros((1, TQ), f32))
    )
    _, _, out = attention_step(None, None, scale, kk, vt, s1, None, scores=False, exps=False)
    ot[TILES - 1] = out
    send_back(3)
    attr[me.head] = atts[me.e]

    w_arrival(0, wf.at[me.sib])
    other = me.sib - me.dp
    w_arrival(5, wf.at[me.left + other])
    w_arrival(6, wf.at[me.right + other])
    w_arrival(7, wf.at[me.opp + other, top_half])
    w_arrival(8, wf.at[me.opp + other, low_half])
    own_w.wait()

    def heads_in(j):
        @pl.when(j != me.head)
        def _():
            arrival(attr.at[j], at_ss.at[j], at_rs.at[j]).wait_recv()

    loop(16, heads_in)

    def project(n):
        rows = jnp.concatenate([attr[j] for j in range(KV)], axis=1)
        product = lax.dot_general(rows, wf[n], (((1,), (0,)), ((), ())), preferred_element_type=f32)
        out_ref[0, :, pl.ds(pl.multiple_of(n * W_COLS, W_COLS), W_COLS)] = product.astype(bf16)

    loop(8, project)

    def sent(n):
        @pl.when(n != me.e)
        def _():
            kv_copy(n).wait_send()
            q_copy(n).wait_send()
            at_copy(n).wait_send()

        fw_copy(n).wait_send()

    loop(16, sent)
    for copy in w_own + w_next + w_last:
        copy.wait_send()


def on_device(queries, keys, values, q_gain, k_gain, w_out):
    cos_table, sin_table = rotary_tables(lax.axis_index("sp") * TOK, TOK)
    q_gains = jnp.broadcast_to(q_gain[:, None], (HD, TOK))
    k_gains = jnp.broadcast_to(k_gain[:, None], (HD, TOK))
    dma = pltpu.SemaphoreType.DMA
    vmem = pl.BlockSpec(memory_space=pltpu.VMEM)
    return pl.pallas_call(
        layer,
        out_shape=jax.ShapeDtypeStruct((1, TOK, W_ROWS), bf16),
        in_specs=[vmem] * 8,
        out_specs=vmem,
        scratch_shapes=[
            pltpu.VMEM((16, TOK, 128), bf16),
            pltpu.VMEM((16, TOK, 128), bf16),
            pltpu.VMEM((2, 16, TOK, 128), bf16),
            pltpu.VMEM((16, TOK, 128), bf16),
            pltpu.VMEM((KEYS, 128), bf16),
            pltpu.VMEM((HD, KEYS), bf16),
            pltpu.VMEM((TILES, 256, TQ), bf16),
            pltpu.VMEM((KEYS, TQ), f32),
            pltpu.VMEM((KEYS, TQ), f32),
            pltpu.VMEM((TILES, HD, TQ), f32),
            pltpu.VMEM((16, TOK, 128), bf16),
            pltpu.VMEM((16, TOK, 128), bf16),
            pltpu.VMEM((8, W_ROWS, W_COLS), bf16),
            dma((16,)), dma((16,)), dma((16,)), dma((16,)),
            dma((16,)), dma((16,)), dma((16,)), dma((16,)),
            dma((9,)), dma((9,)), dma,
        ],
        compiler_params=pltpu.CompilerParams(
            collective_id=0, has_side_effects=True, vmem_limit_bytes=60 * 2**20
        ),
    )(queries, keys, values, w_out, cos_table, sin_table, q_gains, k_gains)


def solution(mesh):
    return jax.shard_map(
        on_device,
        mesh=mesh,
        in_specs=(P("dp", None, "sp"), P("dp", None, "sp"), P("dp", None, "sp"), P(), P(), P(None, "dp")),
        out_specs=P("dp", "sp", None),
        check_vma=False,
    )
```

```python
import jax
import jax.numpy as jnp
from jax import lax
from jax.experimental import pallas as pl
from jax.experimental.pallas import tpu as pltpu
from jax.sharding import PartitionSpec as P

HD = 64
QH = 32
KV = 16
GRID_W = 64
Z = 8
Y = 4
X = 4
TOK = 160
KEYS = 5120
TQ = 256
TILES = 20
KC = 256
GROUP = 4
SPAN = GROUP * TOK
W_ROWS = 2048
W_COLS = 256

epsilon = 1e-06
octaves = -13.287712379549449 / 16
log2_scale = HD ** (-0.5) * 1.4426950408889634
f32 = jnp.float32
bf16 = jnp.bfloat16
MESH = pl.DeviceIdType.MESH


def lanes(rows):
    return lax.broadcasted_iota(jnp.int32, (rows, 2 * HD), 1)


def rotary_tables(first_row):
    lane = lanes(TOK)
    position = first_row + lax.broadcasted_iota(jnp.int32, (TOK, 2 * HD), 0)
    place = jnp.where((lane & 32) == 0, position >> 6, position & (GRID_W - 1)).astype(f32)
    angle = place * jnp.exp2((lane & 15).astype(f32) * octaves)
    sin_table = jnp.sin(angle)
    return jnp.cos(angle), jnp.where((lane & 16) == 0, -sin_table, sin_table)


def head_sums():
    row = lax.broadcasted_iota(jnp.int32, (4 * HD, 2 * HD), 0)
    col = lax.broadcasted_iota(jnp.int32, (4 * HD, 2 * HD), 1)
    return jnp.where(((row >> 6) & 1) == (col >> 6), 1.0, 0.0).astype(bf16)


def turned(u, gain, tables, ones):
    square = u * u
    high = square.astype(bf16)
    low = (square - high.astype(f32)).astype(bf16)
    sums = lax.dot_general(
        jnp.concatenate([high, low], axis=1), ones, (((1,), (0,)), ((), ())), preferred_element_type=f32
    )
    n = u * lax.rsqrt(sums * (1.0 / HD) + epsilon) * gain
    rot = jnp.where(
        (lanes(TOK) & 16) == 0, pltpu.roll(n, 2 * HD - 16, 1), pltpu.roll(n, 16, 1)
    )
    return n * tables[0] + rot * tables[1]


class Place:
    def __init__(self):
        sp = lax.axis_index("sp")
        self.dp = lax.axis_index("dp")
        self.z, self.y = lax.div(sp, Y), lax.rem(sp, Y)
        self.g = lax.div(self.y, 2)
        self.e = self.g * (3 - self.y) + (1 - self.g) * self.y
        self.head = 2 * self.z + self.e
        self.own = 12 + self.e
        self.partner = self.z * Y + 3 - self.y
        x, self.c = lax.div(self.dp, 2), lax.rem(self.dp, 2)
        self.left = lax.rem(x + X - 1, X) * 2 + self.c
        self.right = lax.rem(x + 1, X) * 2 + self.c
        self.sib = self.dp + 1 - 2 * self.c
        self.opp = lax.rem(x + 2, X) * 2 + self.c

    def offset(self, n):
        i = lax.rem(lax.div(n, 2) + 2, Z)
        return lax.div(i + 1, 2) * (2 * lax.rem(i, 2) - 1)

    def at(self, z, e):
        return z * Y + self.g * 3 + e * (1 - 2 * self.g)

    def target_z(self, n):
        return lax.rem(self.z + self.offset(n) + Z, Z)

    def source_z(self, n):
        return lax.rem(self.z - self.offset(n) + Z, Z)

    def slot_there(self, n):
        return 2 * lax.div(n, 2) + self.e


def loop(count, body):
    def step(n, carry):
        body(n)
        return carry

    lax.fori_loop(0, count, step, 0)


def scores_of(k, q):
    return lax.dot_general(k, q, (((1,), (0,)), ((), ())), preferred_element_type=f32)


def by_eight(x):
    return x.reshape(x.shape[0] // 8, 8, TQ)


def attention_step(q, top, scale, kk, vt, x_ref, y_ref, scores=True, exps=True):
    m = jnp.full((8, TQ), -jnp.inf, f32)
    total = jnp.zeros((8, TQ), f32)
    out = None
    tops = jnp.broadcast_to(top, (8, TQ)) if exps else None
    scales = jnp.broadcast_to(scale, (8, TQ))
    zeros = []
    for j in range(KEYS // KC):
        at = slice(j * KC, (j + 1) * KC)
        if exps:
            e = jnp.exp2(by_eight(y_ref[at, :]) - tops)
            y_ref[at, :] = e.reshape(KC, TQ)
            part = jnp.sum(e, axis=0)
            total = total + part
            zeros.append(jnp.minimum(part, 0.0))
        by = scales + zeros[j - 2] if exps and j >= 2 else scales
        weights = (by_eight(x_ref[at, :]) * by).reshape(KC, TQ).astype(bf16)
        part = lax.dot_general(vt[:, at], weights, (((1,), (0,)), ((), ())), preferred_element_type=f32)
        out = part if out is None else out + part
        if scores:
            s = scores_of(kk[at, :], q)
            x_ref[at, :] = s
            m = jnp.maximum(m, jnp.max(by_eight(s), axis=0))
    return m, total, out


def layer(
    q_ref, k_ref, v_ref, w_ref, qg_ref, kg_ref, out_ref,
    kvs, qs, kvr, qr, kk, vt, qt, s0, s1, ot, atts, attr, wf,
    kv_ss, kv_rs, fw_ss, fw_rs, q_ss, q_rs, at_ss, at_rs, w_ss, w_rs, own_sem,
):
    me = Place()

    def remote(src, dst, ss, rs, **device):
        return pltpu.make_async_remote_copy(
            src_ref=src, dst_ref=dst, send_sem=ss, recv_sem=rs, device_id=device, device_id_type=MESH
        )

    barrier = pltpu.get_barrier_semaphore()

    def hello(**device):
        pl.semaphore_signal(barrier, inc=1, device_id=device, device_id_type=MESH)

    def greet(n):
        @pl.when(n != me.own)
        def _():
            hello(sp=me.at(me.target_z(n), lax.rem(n, 2)))

    loop(16, greet)
    hello(sp=me.partner)
    hello(dp=me.sib)
    hello(dp=me.left)
    hello(dp=me.right)

    tables = rotary_tables(lax.axis_index("sp") * TOK)
    ones = head_sums()

    def two_heads(ref):
        gain = ref[...].reshape(1, HD)
        return jnp.concatenate([gain, gain], axis=1)

    q_gain, k_gain = two_heads(qg_ref), two_heads(kg_ref)
    first_head = lanes(TOK) < HD

    def make_kv(i):
        at = pl.ds(pl.multiple_of(me.target_z(2 * i) * 2 * HD, 2 * HD), 2 * HD)
        k = turned(k_ref[0, :, at].astype(f32), k_gain, tables, ones)
        v = v_ref[0, :, at].astype(f32)
        kvs[2 * i] = jnp.where(first_head, k, pltpu.roll(v, HD, 1)).astype(bf16)
        kvs[2 * i + 1] = jnp.where(first_head, pltpu.roll(k, HD, 1), v).astype(bf16)

    def make_q(n):
        j = 2 * me.target_z(n) + lax.rem(n, 2)
        at = pl.ds(pl.multiple_of(j * 2 * HD, 2 * HD), 2 * HD)
        qs[n] = turned(q_ref[0, :, at].astype(f32), q_gain, tables, ones).astype(bf16)

    def kv_copy(n):
        there = me.slot_there(n)
        return remote(
            kvs.at[n], kvr.at[0, there], kv_ss.at[n], kv_rs.at[there],
            sp=me.at(me.target_z(n), lax.rem(n, 2)),
        )

    def q_copy(n):
        there = me.slot_there(n)
        return remote(
            qs.at[n], qr.at[there], q_ss.at[n], q_rs.at[there],
            sp=me.at(me.target_z(n), lax.rem(n, 2)),
        )

    def fw_copy(n):
        return remote(kvr.at[0, n], kvr.at[1, n], fw_ss.at[n], fw_rs.at[n], sp=me.partner)

    def at_copy(n):
        return remote(
            atts.at[n], attr.at[me.head], at_ss.at[n], at_rs.at[me.head],
            sp=me.at(me.source_z(n), lax.rem(n, 2)),
        )

    def arrival(ref, ss, rs):
        return remote(ref, ref, ss, rs, sp=me.partner)

    top_half, low_half = pl.ds(0, W_ROWS // 2), pl.ds(W_ROWS // 2, W_ROWS // 2)

    def w_copy(kind, src, dst, dp):
        return remote(src, dst, w_ss.at[kind], w_rs.at[kind], dp=dp)

    w_own = (
        w_copy(0, w_ref, wf.at[me.dp], me.sib),
        w_copy(1, w_ref, wf.at[me.dp], me.right),
        w_copy(2, w_ref, wf.at[me.dp], me.left),
    )
    w_next = (
        w_copy(3, wf.at[me.left, top_half], wf.at[me.left, top_half], me.right),
        w_copy(4, wf.at[me.right, low_half], wf.at[me.right, low_half], me.left),
        w_copy(5, wf.at[me.left], wf.at[me.left], me.sib),
        w_copy(6, wf.at[me.right], wf.at[me.right], me.sib),
    )
    w_last = (
        w_copy(7, wf.at[me.opp, top_half], wf.at[me.opp, top_half], me.sib),
        w_copy(8, wf.at[me.opp, low_half], wf.at[me.opp, low_half], me.sib),
    )

    def w_arrival(kind, ref):
        arrival(ref, w_ss.at[kind], w_rs.at[kind]).wait_recv()

    def make_four(r):
        make_kv(2 * r)
        make_kv(2 * r + 1)

    loop(4, make_four)
    pl.semaphore_wait(barrier, 19)

    def send_kv(n):
        @pl.when(n != me.own)
        def _():
            kv_copy(n).start()

    loop(16, send_kv)
    kvr[0, me.own] = kvs[me.own]

    def make_q_four(r):
        for n in range(4):
            make_q(4 * r + n)

    loop(4, make_q_four)

    def send_q(n):
        @pl.when(n != me.own)
        def _():
            q_copy(n).start()

    loop(16, send_q)
    qr[me.own] = qs[me.own]
    own_w = pltpu.make_async_copy(w_ref, wf.at[me.dp], own_sem)
    own_w.start()
    for copy in w_own:
        copy.start()

    def forward(n):
        @pl.when(n != me.own)
        def _():
            arrival(kvr.at[0, n], kv_ss.at[n], kv_rs.at[n]).wait_recv()

        fw_copy(n).start()

    loop(16, forward)

    def make_keys(half, g):
        block = kvr[half, pl.ds(GROUP * g, GROUP)].reshape(SPAN, 2 * HD)
        at = pl.ds(pl.multiple_of((half * GROUP + g) * SPAN, 128), SPAN)
        twice = jnp.concatenate([block[:, :HD], block[:, :HD]], axis=1)
        kk[at, :] = twice
        vt[:, at] = jnp.transpose(block)[HD:]
        return at, twice

    def make_queries(g):
        def wait(r):
            n = GROUP * g + r

            @pl.when(n != me.own)
            def _():
                arrival(qr.at[n], q_ss.at[n], q_rs.at[n]).wait_recv()

        loop(4, wait)
        block = qr[pl.ds(GROUP * g, GROUP)].reshape(SPAN, 2 * HD)
        t = jnp.transpose(block.astype(f32)) * log2_scale
        t = jnp.concatenate([t[:HD], t[HD:]], axis=1)
        first = t.astype(bf16)
        second = (t - first.astype(f32)).astype(bf16)
        terms = jnp.concatenate([first, second], axis=0)
        for u in range(5):
            qt[5 * g + u] = terms[:, u * TQ : (u + 1) * TQ]

    def send_back(g):
        tiles = jnp.concatenate([ot[5 * g + u] for u in range(5)], axis=1)
        heads = jnp.concatenate([tiles[:, :SPAN], tiles[:, SPAN:]], axis=0)
        atts[pl.ds(GROUP * g, GROUP)] = jnp.transpose(heads).astype(bf16).reshape(GROUP, TOK, 2 * HD)

        def send(r):
            n = GROUP * g + r

            @pl.when(n != me.own)
            def _():
                at_copy(n).start()

        loop(4, send)

    row_top = lambda m: jnp.max(m, axis=0, keepdims=True)
    row_scale = lambda total: 1.0 / jnp.sum(total, axis=0, keepdims=True)
    s1[...] = jnp.zeros_like(s1)
    make_queries(0)

    def first_scores(half, g, m):
        at, twice = make_keys(half, g)
        s = scores_of(twice, qt[0])
        s0[at, :] = s
        return jnp.maximum(m, jnp.max(by_eight(s), axis=0))

    def partner_keys(g, m):
        def wait(n):
            arrival(kvr.at[1, GROUP * g + n], fw_ss.at[GROUP * g + n], fw_rs.at[GROUP * g + n]).wait_recv()

        loop(4, wait)
        return first_scores(1, g, m)

    m = jnp.full((8, TQ), -jnp.inf, f32)
    m = lax.fori_loop(0, 4, lambda g, m: first_scores(0, g, m), m)
    m = lax.fori_loop(0, 4, partner_keys, m)

    def two_tiles(p, carry):
        top, scale = carry

        @pl.when(jnp.logical_or(p == 2, jnp.logical_or(p == 4, p == 7)))
        def _():
            make_queries(lax.div(p, 2))

        @pl.when(p == 3)
        def _():
            w_arrival(1, wf.at[me.left])
            w_arrival(2, wf.at[me.right])
            for copy in w_next:
                copy.start()

        @pl.when(p == 8)
        def _():
            w_arrival(3, wf.at[me.opp, top_half])
            w_arrival(4, wf.at[me.opp, low_half])
            for copy in w_last:
                copy.start()

        m, total, out = attention_step(qt[2 * p + 1], top, scale, kk, vt, s1, s0)
        ot[jnp.maximum(2 * p - 1, 0)] = out
        top, scale = row_top(m), row_scale(total)
        m, total, out = attention_step(
            qt[jnp.minimum(2 * p + 2, TILES - 1)], top, scale, kk, vt, s0, s1
        )
        ot[2 * p] = out

        @pl.when(jnp.logical_or(p == 2, jnp.logical_or(p == 5, p == 7)))
        def _():
            send_back(lax.div(p, 3))

        return row_top(m), row_scale(total)

    _, scale = lax.fori_loop(
        0, TILES // 2, two_tiles, (row_top(m), jnp.zeros((1, TQ), f32))
    )
    _, _, out = attention_step(None, None, scale, kk, vt, s1, None, scores=False, exps=False)
    ot[TILES - 1] = out
    send_back(3)
    attr[me.head] = atts[me.own]

    w_arrival(0, wf.at[me.sib])
    other = me.sib - me.dp
    w_arrival(5, wf.at[me.left + other])
    w_arrival(6, wf.at[me.right + other])
    w_arrival(7, wf.at[me.opp + other, top_half])
    w_arrival(8, wf.at[me.opp + other, low_half])
    own_w.wait()

    def heads_in(j):
        @pl.when(j != me.head)
        def _():
            arrival(attr.at[j], at_ss.at[j], at_rs.at[j]).wait_recv()

    loop(16, heads_in)

    def project(n):
        rows = jnp.concatenate([attr[j] for j in range(KV)], axis=1)
        product = lax.dot_general(rows, wf[n], (((1,), (0,)), ((), ())), preferred_element_type=f32)
        out_ref[0, :, pl.ds(pl.multiple_of(n * W_COLS, W_COLS), W_COLS)] = product.astype(bf16)

    loop(8, project)

    def sent(n):
        @pl.when(n != me.own)
        def _():
            kv_copy(n).wait_send()
            q_copy(n).wait_send()
            at_copy(n).wait_send()

        fw_copy(n).wait_send()

    loop(16, sent)
    for copy in w_own + w_next + w_last:
        copy.wait_send()


def on_device(queries, keys, values, q_gain, k_gain, w_out):
    dma = pltpu.SemaphoreType.DMA
    vmem = pl.BlockSpec(memory_space=pltpu.VMEM)
    return pl.pallas_call(
        layer,
        out_shape=jax.ShapeDtypeStruct((1, TOK, W_ROWS), bf16),
        in_specs=[vmem] * 6,
        out_specs=vmem,
        scratch_shapes=[
            pltpu.VMEM((16, TOK, 128), bf16),
            pltpu.VMEM((16, TOK, 128), bf16),
            pltpu.VMEM((2, 16, TOK, 128), bf16),
            pltpu.VMEM((16, TOK, 128), bf16),
            pltpu.VMEM((KEYS, 128), bf16),
            pltpu.VMEM((HD, KEYS), bf16),
            pltpu.VMEM((TILES, 2 * HD, TQ), bf16),
            pltpu.VMEM((KEYS, TQ), f32),
            pltpu.VMEM((KEYS, TQ), f32),
            pltpu.VMEM((TILES, HD, TQ), f32),
            pltpu.VMEM((16, TOK, 128), bf16),
            pltpu.VMEM((16, TOK, 128), bf16),
            pltpu.VMEM((8, W_ROWS, W_COLS), bf16),
            dma((16,)), dma((16,)), dma((16,)), dma((16,)),
            dma((16,)), dma((16,)), dma((16,)), dma((16,)),
            dma((9,)), dma((9,)), dma,
        ],
        compiler_params=pltpu.CompilerParams(
            collective_id=0, has_side_effects=True, vmem_limit_bytes=60 * 2**20
        ),
    )(
        jnp.swapaxes(queries, 1, 2),
        jnp.swapaxes(keys, 1, 2),
        jnp.swapaxes(values, 1, 2),
        w_out,
        q_gain,
        k_gain,
    )


def solution(mesh):
    return jax.shard_map(
        on_device,
        mesh=mesh,
        in_specs=(P("dp", None, "sp"), P("dp", None, "sp"), P("dp", None, "sp"), P(), P(), P(None, "dp")),
        out_specs=P("dp", "sp", None),
        check_vma=False,
    )
```

```python
import jax
import jax.numpy as jnp
from jax import lax
from jax.experimental import pallas as pl
from jax.experimental.pallas import tpu as pltpu
from jax.sharding import PartitionSpec as P

HD = 64
QH = 32
KV = 16
GRID_W = 64
Z = 8
Y = 4
X = 4
TOK = 160
KEYS = 5120
TQ = 256
TILES = 20
KC = 256
GROUP = 4
SPAN = GROUP * TOK
W_ROWS = 2048
W_COLS = 256

epsilon = 1e-06
octaves = -13.287712379549449 / 16
log2_scale = HD ** (-0.5) * 1.4426950408889634
f32 = jnp.float32
bf16 = jnp.bfloat16
MESH = pl.DeviceIdType.MESH


def lanes(rows):
    return lax.broadcasted_iota(jnp.int32, (rows, 2 * HD), 1)


def rotary_tables(first_row):
    lane = lanes(TOK)
    position = first_row + lax.broadcasted_iota(jnp.int32, (TOK, 2 * HD), 0)
    place = jnp.where((lane & 32) == 0, position >> 6, position & (GRID_W - 1)).astype(f32)
    angle = place * jnp.exp2((lane & 15).astype(f32) * octaves)
    sin_table = jnp.sin(angle)
    return jnp.cos(angle), jnp.where((lane & 16) == 0, -sin_table, sin_table)


def head_sums():
    row = lax.broadcasted_iota(jnp.int32, (4 * HD, 2 * HD), 0)
    col = lax.broadcasted_iota(jnp.int32, (4 * HD, 2 * HD), 1)
    return jnp.where(((row >> 6) & 1) == (col >> 6), 1.0, 0.0).astype(bf16)


def turned(u, gain, tables, ones):
    square = u * u
    high = square.astype(bf16)
    low = (square - high.astype(f32)).astype(bf16)
    sums = lax.dot_general(
        jnp.concatenate([high, low], axis=1), ones, (((1,), (0,)), ((), ())), preferred_element_type=f32
    )
    n = u * lax.rsqrt(sums * (1.0 / HD) + epsilon) * gain
    rot = jnp.where(
        (lanes(TOK) & 16) == 0, pltpu.roll(n, 2 * HD - 16, 1), pltpu.roll(n, 16, 1)
    )
    return n * tables[0] + rot * tables[1]


def div(a, b):
    return a // b if isinstance(a, int) else lax.div(a, b)


def rem(a, b):
    return a % b if isinstance(a, int) else lax.rem(a, b)


class Place:
    def __init__(self):
        sp = lax.axis_index("sp")
        self.dp = lax.axis_index("dp")
        self.z, self.y = lax.div(sp, Y), lax.rem(sp, Y)
        self.g = lax.div(self.y, 2)
        self.e = self.g * (3 - self.y) + (1 - self.g) * self.y
        self.head = 2 * self.z + self.e
        self.own = 12 + self.e
        self.partner = self.z * Y + 3 - self.y
        x, self.c = lax.div(self.dp, 2), lax.rem(self.dp, 2)
        self.left = lax.rem(x + X - 1, X) * 2 + self.c
        self.right = lax.rem(x + 1, X) * 2 + self.c
        self.sib = self.dp + 1 - 2 * self.c
        self.opp = lax.rem(x + 2, X) * 2 + self.c

    def offset(self, n):
        i = rem(div(n, 2) + 2, Z)
        return div(i + 1, 2) * (2 * rem(i, 2) - 1)

    def at(self, z, e):
        return z * Y + self.g * 3 + e * (1 - 2 * self.g)

    def target_z(self, n):
        return lax.rem(self.z + self.offset(n) + Z, Z)

    def source_z(self, n):
        return lax.rem(self.z - self.offset(n) + Z, Z)

    def slot_there(self, n):
        return 2 * div(n, 2) + self.e


def all_slots(me, body):
    for n in range(16):
        if n in (12, 13):
            pl.when(n != me.own)(lambda n=n: body(n))
        else:
            body(n)


def loop(count, body):
    def step(n, carry):
        body(n)
        return carry

    lax.fori_loop(0, count, step, 0)


def scores_of(k, q):
    return lax.dot_general(k, q, (((1,), (0,)), ((), ())), preferred_element_type=f32)


def by_eight(x):
    return x.reshape(x.shape[0] // 8, 8, TQ)


def attention_step(q, top, scale, kk, vt, x_ref, y_ref, scores=True, exps=True):
    m = jnp.full((8, TQ), -jnp.inf, f32)
    total = jnp.zeros((8, TQ), f32)
    out = None
    tops = jnp.broadcast_to(top, (8, TQ)) if exps else None
    scales = jnp.broadcast_to(scale, (8, TQ))
    zeros = []
    for j in range(KEYS // KC):
        at = slice(j * KC, (j + 1) * KC)
        if exps:
            e = jnp.exp2(by_eight(y_ref[at, :]) - tops)
            y_ref[at, :] = e.reshape(KC, TQ)
            part = jnp.sum(e, axis=0)
            total = total + part
            zeros.append(jnp.minimum(part, 0.0))
        by = scales + zeros[j - 2] if exps and j >= 2 else scales
        weights = (by_eight(x_ref[at, :]) * by).reshape(KC, TQ).astype(bf16)
        part = lax.dot_general(vt[:, at], weights, (((1,), (0,)), ((), ())), preferred_element_type=f32)
        out = part if out is None else out + part
        if scores:
            s = scores_of(kk[at, :], q)
            x_ref[at, :] = s
            m = jnp.maximum(m, jnp.max(by_eight(s), axis=0))
    return m, total, out


def layer(
    q_ref, k_ref, v_ref, w_ref, qg_ref, kg_ref, out_ref,
    kvs, qs, kvr, qr, kk, vt, qt, s0, s1, ot, atts, attr, wf,
    kv_ss, kv_rs, fw_ss, fw_rs, q_ss, q_rs, at_ss, at_rs, w_ss, w_rs, own_sem,
    k_in, v_in, q_in, in_sem,
):
    me = Place()

    def remote(src, dst, ss, rs, **device):
        return pltpu.make_async_remote_copy(
            src_ref=src, dst_ref=dst, send_sem=ss, recv_sem=rs, device_id=device, device_id_type=MESH
        )

    barrier = pltpu.get_barrier_semaphore()

    def hello(**device):
        pl.semaphore_signal(barrier, inc=1, device_id=device, device_id_type=MESH)

    inputs = [
        pltpu.make_async_copy(src.at[0], dst, in_sem.at[n])
        for n, (src, dst) in enumerate(((k_ref, k_in), (v_ref, v_in), (q_ref, q_in)))
    ]
    for copy in inputs:
        copy.start()
    all_slots(me, lambda n: hello(sp=me.at(me.target_z(n), rem(n, 2))))
    hello(sp=me.partner)
    hello(dp=me.sib)
    hello(dp=me.left)
    hello(dp=me.right)

    tables = rotary_tables(lax.axis_index("sp") * TOK)
    ones = head_sums()

    def two_heads(ref):
        gain = ref[...].reshape(1, HD)
        return jnp.concatenate([gain, gain], axis=1)

    q_gain, k_gain = two_heads(qg_ref), two_heads(kg_ref)
    first_head = lanes(TOK) < HD

    def make_kv(i):
        at = pl.ds(pl.multiple_of(me.target_z(2 * i) * 2 * HD, 2 * HD), 2 * HD)
        k = turned(k_in[:, at].astype(f32), k_gain, tables, ones)
        v = v_in[:, at].astype(f32)
        kvs[2 * i] = jnp.where(first_head, k, pltpu.roll(v, HD, 1)).astype(bf16)
        kvs[2 * i + 1] = jnp.where(first_head, pltpu.roll(k, HD, 1), v).astype(bf16)

    def make_q(n):
        j = 2 * me.target_z(n) + rem(n, 2)
        at = pl.ds(pl.multiple_of(j * 2 * HD, 2 * HD), 2 * HD)
        qs[n] = turned(q_in[:, at].astype(f32), q_gain, tables, ones).astype(bf16)

    def kv_copy(n):
        there = me.slot_there(n)
        return remote(
            kvs.at[n], kvr.at[0, there], kv_ss.at[n], kv_rs.at[there],
            sp=me.at(me.target_z(n), rem(n, 2)),
        )

    def q_copy(n):
        there = me.slot_there(n)
        return remote(
            qs.at[n], qr.at[there], q_ss.at[n], q_rs.at[there],
            sp=me.at(me.target_z(n), rem(n, 2)),
        )

    def fw_copy(n):
        return remote(kvr.at[0, n], kvr.at[1, n], fw_ss.at[n], fw_rs.at[n], sp=me.partner)

    def at_copy(n):
        return remote(
            atts.at[n], attr.at[me.head], at_ss.at[n], at_rs.at[me.head],
            sp=me.at(me.source_z(n), rem(n, 2)),
        )

    def arrival(ref, ss, rs):
        return remote(ref, ref, ss, rs, sp=me.partner)

    top_half, low_half = pl.ds(0, W_ROWS // 2), pl.ds(W_ROWS // 2, W_ROWS // 2)

    def w_copy(kind, src, dst, dp):
        return remote(src, dst, w_ss.at[kind], w_rs.at[kind], dp=dp)

    w_own = (
        w_copy(0, w_ref, wf.at[me.dp], me.sib),
        w_copy(1, w_ref, wf.at[me.dp], me.right),
        w_copy(2, w_ref, wf.at[me.dp], me.left),
    )
    w_next = (
        w_copy(3, wf.at[me.left, top_half], wf.at[me.left, top_half], me.right),
        w_copy(4, wf.at[me.right, low_half], wf.at[me.right, low_half], me.left),
        w_copy(5, wf.at[me.left], wf.at[me.left], me.sib),
        w_copy(6, wf.at[me.right], wf.at[me.right], me.sib),
    )
    w_last = (
        w_copy(7, wf.at[me.opp, top_half], wf.at[me.opp, top_half], me.sib),
        w_copy(8, wf.at[me.opp, low_half], wf.at[me.opp, low_half], me.sib),
    )

    def w_arrival(kind, ref):
        arrival(ref, w_ss.at[kind], w_rs.at[kind]).wait_recv()

    def make_four(r):
        make_kv(2 * r)
        make_kv(2 * r + 1)

    inputs[0].wait()
    inputs[1].wait()
    loop(4, make_four)
    pl.semaphore_wait(barrier, 19)

    all_slots(me, lambda n: kv_copy(n).start())
    kvr[0, me.own] = kvs[me.own]

    def make_q_four(r):
        for n in range(4):
            make_q(4 * r + n)

    inputs[2].wait()
    loop(4, make_q_four)

    all_slots(me, lambda n: q_copy(n).start())
    qr[me.own] = qs[me.own]
    own_w = pltpu.make_async_copy(w_ref, wf.at[me.dp], own_sem)
    own_w.start()
    for copy in w_own:
        copy.start()

    def forward(n):
        @pl.when(n != me.own)
        def _():
            arrival(kvr.at[0, n], kv_ss.at[n], kv_rs.at[n]).wait_recv()

        fw_copy(n).start()

    loop(16, forward)

    def make_keys(half, g):
        block = kvr[half, pl.ds(GROUP * g, GROUP)].reshape(SPAN, 2 * HD)
        at = pl.ds(pl.multiple_of((half * GROUP + g) * SPAN, 128), SPAN)
        twice = jnp.concatenate([block[:, :HD], block[:, :HD]], axis=1)
        kk[at, :] = twice
        vt[:, at] = jnp.transpose(block)[HD:]
        return at, twice

    def make_queries(g):
        def wait(r):
            n = GROUP * g + r

            @pl.when(n != me.own)
            def _():
                arrival(qr.at[n], q_ss.at[n], q_rs.at[n]).wait_recv()

        loop(4, wait)
        block = qr[pl.ds(GROUP * g, GROUP)].reshape(SPAN, 2 * HD)
        t = jnp.transpose(block.astype(f32)) * log2_scale
        t = jnp.concatenate([t[:HD], t[HD:]], axis=1)
        first = t.astype(bf16)
        second = (t - first.astype(f32)).astype(bf16)
        terms = jnp.concatenate([first, second], axis=0)
        for u in range(5):
            qt[5 * g + u] = terms[:, u * TQ : (u + 1) * TQ]

    def send_back(g):
        tiles = jnp.concatenate([ot[5 * g + u] for u in range(5)], axis=1)
        heads = jnp.concatenate([tiles[:, :SPAN], tiles[:, SPAN:]], axis=0)
        atts[pl.ds(GROUP * g, GROUP)] = jnp.transpose(heads).astype(bf16).reshape(GROUP, TOK, 2 * HD)

        def send(r):
            n = GROUP * g + r

            @pl.when(n != me.own)
            def _():
                at_copy(n).start()

        loop(4, send)

    row_top = lambda m: jnp.max(m, axis=0, keepdims=True)
    row_scale = lambda total: 1.0 / jnp.sum(total, axis=0, keepdims=True)
    s1[...] = jnp.zeros_like(s1)
    make_queries(0)

    def first_scores(half, g, m):
        at, twice = make_keys(half, g)
        s = scores_of(twice, qt[0])
        s0[at, :] = s
        return jnp.maximum(m, jnp.max(by_eight(s), axis=0))

    def partner_keys(g, m):
        def wait(n):
            arrival(kvr.at[1, GROUP * g + n], fw_ss.at[GROUP * g + n], fw_rs.at[GROUP * g + n]).wait_recv()

        loop(4, wait)
        return first_scores(1, g, m)

    m = jnp.full((8, TQ), -jnp.inf, f32)
    m = lax.fori_loop(0, 4, lambda g, m: first_scores(0, g, m), m)
    m = lax.fori_loop(0, 4, partner_keys, m)

    def two_tiles(p, carry):
        top, scale = carry

        @pl.when(jnp.logical_or(p == 2, jnp.logical_or(p == 4, p == 7)))
        def _():
            make_queries(lax.div(p, 2))

        m, total, out = attention_step(qt[2 * p + 1], top, scale, kk, vt, s1, s0)
        ot[jnp.maximum(2 * p - 1, 0)] = out
        top, scale = row_top(m), row_scale(total)

        @pl.when(p == 3)
        def _():
            w_arrival(1, wf.at[me.left])
            w_arrival(2, wf.at[me.right])
            for copy in w_next:
                copy.start()

        @pl.when(p == 8)
        def _():
            w_arrival(3, wf.at[me.opp, top_half])
            w_arrival(4, wf.at[me.opp, low_half])
            for copy in w_last:
                copy.start()

        m, total, out = attention_step(
            qt[jnp.minimum(2 * p + 2, TILES - 1)], top, scale, kk, vt, s0, s1
        )
        ot[2 * p] = out

        @pl.when(jnp.logical_or(p == 2, jnp.logical_or(p == 5, p == 7)))
        def _():
            send_back(lax.div(p, 3))

        return row_top(m), row_scale(total)

    _, scale = lax.fori_loop(
        0, TILES // 2, two_tiles, (row_top(m), jnp.zeros((1, TQ), f32))
    )
    _, _, out = attention_step(None, None, scale, kk, vt, s1, None, scores=False, exps=False)
    ot[TILES - 1] = out
    send_back(3)
    attr[me.head] = atts[me.own]

    w_arrival(0, wf.at[me.sib])
    other = me.sib - me.dp
    w_arrival(5, wf.at[me.left + other])
    w_arrival(6, wf.at[me.right + other])
    w_arrival(7, wf.at[me.opp + other, top_half])
    w_arrival(8, wf.at[me.opp + other, low_half])
    own_w.wait()

    def heads_in(j):
        @pl.when(j != me.head)
        def _():
            arrival(attr.at[j], at_ss.at[j], at_rs.at[j]).wait_recv()

    loop(16, heads_in)

    def project(n):
        rows = jnp.concatenate([attr[j] for j in range(KV)], axis=1)
        product = lax.dot_general(rows, wf[n], (((1,), (0,)), ((), ())), preferred_element_type=f32)
        out_ref[0, :, pl.ds(pl.multiple_of(n * W_COLS, W_COLS), W_COLS)] = product.astype(bf16)

    loop(8, project)

    def sent(n):
        @pl.when(n != me.own)
        def _():
            kv_copy(n).wait_send()
            q_copy(n).wait_send()
            at_copy(n).wait_send()

        fw_copy(n).wait_send()

    loop(16, sent)
    for copy in w_own + w_next + w_last:
        copy.wait_send()


def on_device(queries, keys, values, q_gain, k_gain, w_out):
    dma = pltpu.SemaphoreType.DMA
    vmem = pl.BlockSpec(memory_space=pltpu.VMEM)
    anywhere = pl.BlockSpec(memory_space=pl.ANY)
    return pl.pallas_call(
        layer,
        out_shape=jax.ShapeDtypeStruct((1, TOK, W_ROWS), bf16),
        in_specs=[anywhere] * 4 + [vmem] * 2,
        out_specs=vmem,
        scratch_shapes=[
            pltpu.VMEM((16, TOK, 128), bf16),
            pltpu.VMEM((16, TOK, 128), bf16),
            pltpu.VMEM((2, 16, TOK, 128), bf16),
            pltpu.VMEM((16, TOK, 128), bf16),
            pltpu.VMEM((KEYS, 128), bf16),
            pltpu.VMEM((HD, KEYS), bf16),
            pltpu.VMEM((TILES, 2 * HD, TQ), bf16),
            pltpu.VMEM((KEYS, TQ), f32),
            pltpu.VMEM((KEYS, TQ), f32),
            pltpu.VMEM((TILES, HD, TQ), f32),
            pltpu.VMEM((16, TOK, 128), bf16),
            pltpu.VMEM((16, TOK, 128), bf16),
            pltpu.VMEM((8, W_ROWS, W_COLS), bf16),
            dma((16,)), dma((16,)), dma((16,)), dma((16,)),
            dma((16,)), dma((16,)), dma((16,)), dma((16,)),
            dma((9,)), dma((9,)), dma,
            pltpu.VMEM((TOK, KV * HD), bf16),
            pltpu.VMEM((TOK, KV * HD), bf16),
            pltpu.VMEM((TOK, QH * HD), bf16),
            dma((3,)),
        ],
        compiler_params=pltpu.CompilerParams(
            collective_id=0, has_side_effects=True, vmem_limit_bytes=60 * 2**20
        ),
    )(
        jnp.swapaxes(queries, 1, 2),
        jnp.swapaxes(keys, 1, 2),
        jnp.swapaxes(values, 1, 2),
        w_out,
        q_gain,
        k_gain,
    )


def solution(mesh):
    return jax.shard_map(
        on_device,
        mesh=mesh,
        in_specs=(P("dp", None, "sp"), P("dp", None, "sp"), P("dp", None, "sp"), P(), P(), P(None, "dp")),
        out_specs=P("dp", "sp", None),
        check_vma=False,
    )
```

```python
import jax
import jax.numpy as jnp
from jax import lax
from jax.experimental import pallas as pl
from jax.experimental.pallas import tpu as pltpu
from jax.sharding import PartitionSpec as P

HD = 64
QH = 32
KV = 16
GRID_W = 64
Z = 8
Y = 4
X = 4
TOK = 160
KEYS = 5120
TQ = 256
TILES = 20
KC = 256
GROUP = 4
SPAN = GROUP * TOK
W_ROWS = 2048
W_COLS = 256

epsilon = 1e-06
octaves = -13.287712379549449 / 16
log2_scale = HD ** (-0.5) * 1.4426950408889634
f32 = jnp.float32
bf16 = jnp.bfloat16
MESH = pl.DeviceIdType.MESH


def lanes(rows):
    return lax.broadcasted_iota(jnp.int32, (rows, 2 * HD), 1)


def rotary_tables(first_row):
    lane = lanes(TOK)
    position = first_row + lax.broadcasted_iota(jnp.int32, (TOK, 2 * HD), 0)
    place = jnp.where((lane & 32) == 0, position >> 6, position & (GRID_W - 1)).astype(f32)
    angle = place * jnp.exp2((lane & 15).astype(f32) * octaves)
    sin_table = jnp.sin(angle)
    return jnp.cos(angle), jnp.where((lane & 16) == 0, -sin_table, sin_table)


def head_sums():
    row = lax.broadcasted_iota(jnp.int32, (4 * HD, 2 * HD), 0)
    col = lax.broadcasted_iota(jnp.int32, (4 * HD, 2 * HD), 1)
    return jnp.where(((row >> 6) & 1) == (col >> 6), 1.0, 0.0).astype(bf16)


def turned(u, gain, tables, ones):
    square = u * u
    high = square.astype(bf16)
    low = (square - high.astype(f32)).astype(bf16)
    sums = lax.dot_general(
        jnp.concatenate([high, low], axis=1), ones, (((1,), (0,)), ((), ())), preferred_element_type=f32
    )
    n = u * lax.rsqrt(sums * (1.0 / HD) + epsilon) * gain
    rot = jnp.where(
        (lanes(TOK) & 16) == 0, pltpu.roll(n, 2 * HD - 16, 1), pltpu.roll(n, 16, 1)
    )
    return n * tables[0] + rot * tables[1]


def div(a, b):
    return a // b if isinstance(a, int) else lax.div(a, b)


def rem(a, b):
    return a % b if isinstance(a, int) else lax.rem(a, b)


class Place:
    def __init__(self):
        sp = lax.axis_index("sp")
        self.dp = lax.axis_index("dp")
        self.z, self.y = lax.div(sp, Y), lax.rem(sp, Y)
        self.g = lax.div(self.y, 2)
        self.e = self.g * (3 - self.y) + (1 - self.g) * self.y
        self.head = 2 * self.z + self.e
        self.own = 12 + self.e
        self.partner = self.z * Y + 3 - self.y
        x, self.c = lax.div(self.dp, 2), lax.rem(self.dp, 2)
        self.left = lax.rem(x + X - 1, X) * 2 + self.c
        self.right = lax.rem(x + 1, X) * 2 + self.c
        self.sib = self.dp + 1 - 2 * self.c
        self.opp = lax.rem(x + 2, X) * 2 + self.c

    def offset(self, n):
        i = rem(div(n, 2) + 2, Z)
        return div(i + 1, 2) * (2 * rem(i, 2) - 1)

    def at(self, z, e):
        return z * Y + self.g * 3 + e * (1 - 2 * self.g)

    def target_z(self, n):
        return lax.rem(self.z + self.offset(n) + Z, Z)

    def source_z(self, n):
        return lax.rem(self.z - self.offset(n) + Z, Z)

    def slot_there(self, n):
        return 2 * div(n, 2) + self.e


def all_slots(me, body):
    for n in range(16):
        if n in (12, 13):
            pl.when(n != me.own)(lambda n=n: body(n))
        else:
            body(n)


def loop(count, body):
    def step(n, carry):
        body(n)
        return carry

    lax.fori_loop(0, count, step, 0)


def scores_of(k, q):
    return lax.dot_general(k, q, (((1,), (0,)), ((), ())), preferred_element_type=f32)


def by_eight(x):
    return x.reshape(x.shape[0] // 8, 8, TQ)


def attention_step(q, top, scale, kk, vt, x_ref, y_ref, scores=True, exps=True):
    m = jnp.full((8, TQ), -jnp.inf, f32)
    total = jnp.zeros((8, TQ), f32)
    out = None
    tops = jnp.broadcast_to(top, (8, TQ)) if exps else None
    scales = jnp.broadcast_to(scale, (8, TQ))
    zeros = []
    for j in range(KEYS // KC):
        at = slice(j * KC, (j + 1) * KC)
        if exps:
            e = jnp.exp2(by_eight(y_ref[at, :]) - tops)
            y_ref[at, :] = e.reshape(KC, TQ)
            part = jnp.sum(e, axis=0)
            total = total + part
            zeros.append(jnp.minimum(part, 0.0))
        by = scales + zeros[j - 2] if exps and j >= 2 else scales
        weights = (by_eight(x_ref[at, :]) * by).reshape(KC, TQ).astype(bf16)
        part = lax.dot_general(vt[:, at], weights, (((1,), (0,)), ((), ())), preferred_element_type=f32)
        out = part if out is None else out + part
        if scores:
            s = scores_of(kk[at, :], q)
            x_ref[at, :] = s
            m = jnp.maximum(m, jnp.max(by_eight(s), axis=0))
    return m, total, out


def layer(
    q_ref, k_ref, v_ref, w_ref, qg_ref, kg_ref, out_ref,
    kvs, qs, kvr, qr, kk, vt, qt, s0, s1, ot, atts, attr, wf,
    kv_ss, kv_rs, fw_ss, fw_rs, q_ss, q_rs, at_ss, at_rs, w_ss, w_rs, own_sem,
    k_in, v_in, q_in, in_sem,
):
    me = Place()

    def remote(src, dst, ss, rs, **device):
        return pltpu.make_async_remote_copy(
            src_ref=src, dst_ref=dst, send_sem=ss, recv_sem=rs, device_id=device, device_id_type=MESH
        )

    barrier = pltpu.get_barrier_semaphore()

    def hello(**device):
        pl.semaphore_signal(barrier, inc=1, device_id=device, device_id_type=MESH)

    inputs = [
        pltpu.make_async_copy(src.at[0], dst, in_sem.at[n])
        for n, (src, dst) in enumerate(((k_ref, k_in), (v_ref, v_in), (q_ref, q_in)))
    ]
    for copy in inputs:
        copy.start()
    all_slots(me, lambda n: hello(sp=me.at(me.target_z(n), rem(n, 2))))
    hello(sp=me.partner)
    hello(dp=me.sib)
    hello(dp=me.left)
    hello(dp=me.right)

    tables = rotary_tables(lax.axis_index("sp") * TOK)
    ones = head_sums()

    def two_heads(ref):
        gain = ref[...].reshape(1, HD)
        return jnp.concatenate([gain, gain], axis=1)

    q_gain, k_gain = two_heads(qg_ref), two_heads(kg_ref)
    first_head = lanes(TOK) < HD

    def make_kv(i):
        at = pl.ds(pl.multiple_of(me.target_z(2 * i) * 2 * HD, 2 * HD), 2 * HD)
        k = turned(k_in[:, at].astype(f32), k_gain, tables, ones)
        v = v_in[:, at].astype(f32)
        kvs[2 * i] = jnp.where(first_head, k, pltpu.roll(v, HD, 1)).astype(bf16)
        kvs[2 * i + 1] = jnp.where(first_head, pltpu.roll(k, HD, 1), v).astype(bf16)

    def make_q(n):
        j = 2 * me.target_z(n) + rem(n, 2)
        at = pl.ds(pl.multiple_of(j * 2 * HD, 2 * HD), 2 * HD)
        qs[n] = turned(q_in[:, at].astype(f32), q_gain, tables, ones).astype(bf16)

    def kv_copy(n):
        there = me.slot_there(n)
        return remote(
            kvs.at[n], kvr.at[0, there], kv_ss.at[n], kv_rs.at[there],
            sp=me.at(me.target_z(n), rem(n, 2)),
        )

    def q_copy(n):
        there = me.slot_there(n)
        return remote(
            qs.at[n], qr.at[there], q_ss.at[n], q_rs.at[there],
            sp=me.at(me.target_z(n), rem(n, 2)),
        )

    def fw_copy(n):
        return remote(kvr.at[0, n], kvr.at[1, n], fw_ss.at[n], fw_rs.at[n], sp=me.partner)

    def at_copy(n):
        return remote(
            atts.at[n], attr.at[me.head], at_ss.at[n], at_rs.at[me.head],
            sp=me.at(me.source_z(n), rem(n, 2)),
        )

    def arrival(ref, ss, rs):
        return remote(ref, ref, ss, rs, sp=me.partner)

    top_half, low_half = pl.ds(0, W_ROWS // 2), pl.ds(W_ROWS // 2, W_ROWS // 2)

    def w_copy(kind, src, dst, dp):
        return remote(src, dst, w_ss.at[kind], w_rs.at[kind], dp=dp)

    w_own = (
        w_copy(0, w_ref, wf.at[me.dp], me.sib),
        w_copy(1, w_ref, wf.at[me.dp], me.right),
        w_copy(2, w_ref, wf.at[me.dp], me.left),
    )
    w_next = (
        w_copy(3, wf.at[me.left, top_half], wf.at[me.left, top_half], me.right),
        w_copy(4, wf.at[me.right, low_half], wf.at[me.right, low_half], me.left),
        w_copy(5, wf.at[me.left], wf.at[me.left], me.sib),
        w_copy(6, wf.at[me.right], wf.at[me.right], me.sib),
    )
    w_last = (
        w_copy(7, wf.at[me.opp, top_half], wf.at[me.opp, top_half], me.sib),
        w_copy(8, wf.at[me.opp, low_half], wf.at[me.opp, low_half], me.sib),
    )

    def w_arrival(kind, ref):
        arrival(ref, w_ss.at[kind], w_rs.at[kind]).wait_recv()

    def make_four(r):
        make_kv(2 * r)
        make_kv(2 * r + 1)

    inputs[0].wait()
    inputs[1].wait()
    loop(4, make_four)
    pl.semaphore_wait(barrier, 19)

    all_slots(me, lambda n: kv_copy(n).start())
    kvr[0, me.own] = kvs[me.own]

    def make_q_four(r):
        for n in range(4):
            make_q(4 * r + n)

    inputs[2].wait()
    loop(4, make_q_four)

    all_slots(me, lambda n: q_copy(n).start())
    qr[me.own] = qs[me.own]
    own_w = pltpu.make_async_copy(w_ref, wf.at[me.dp], own_sem)
    own_w.start()
    for copy in w_own:
        copy.start()

    def forward(n):
        @pl.when(n != me.own)
        def _():
            arrival(kvr.at[0, n], kv_ss.at[n], kv_rs.at[n]).wait_recv()

        fw_copy(n).start()

    loop(16, forward)

    def make_keys(half, g):
        block = kvr[half, pl.ds(GROUP * g, GROUP)].reshape(SPAN, 2 * HD)
        at = pl.ds(pl.multiple_of((half * GROUP + g) * SPAN, 128), SPAN)
        twice = jnp.concatenate([block[:, :HD], block[:, :HD]], axis=1)
        kk[at, :] = twice
        vt[:, at] = jnp.transpose(block)[HD:]
        return at, twice

    def make_queries(g):
        def wait(r):
            n = GROUP * g + r

            @pl.when(n != me.own)
            def _():
                arrival(qr.at[n], q_ss.at[n], q_rs.at[n]).wait_recv()

        loop(4, wait)
        block = qr[pl.ds(GROUP * g, GROUP)].reshape(SPAN, 2 * HD)
        t = jnp.transpose(block.astype(f32)) * log2_scale
        t = jnp.concatenate([t[:HD], t[HD:]], axis=1)
        first = t.astype(bf16)
        second = (t - first.astype(f32)).astype(bf16)
        terms = jnp.concatenate([first, second], axis=0)
        for u in range(5):
            qt[5 * g + u] = terms[:, u * TQ : (u + 1) * TQ]

    def send_back(g):
        tiles = jnp.concatenate([ot[5 * g + u] for u in range(5)], axis=1)
        heads = jnp.concatenate([tiles[:, :SPAN], tiles[:, SPAN:]], axis=0)
        atts[pl.ds(GROUP * g, GROUP)] = jnp.transpose(heads).astype(bf16).reshape(GROUP, TOK, 2 * HD)

        def send(r):
            n = GROUP * g + r

            @pl.when(n != me.own)
            def _():
                at_copy(n).start()

        loop(4, send)

    row_top = lambda m: jnp.max(m, axis=0, keepdims=True)
    row_scale = lambda total: 1.0 / jnp.sum(total, axis=0, keepdims=True)
    s1[...] = jnp.zeros_like(s1)
    make_queries(0)

    def first_scores(half, g, m):
        at, twice = make_keys(half, g)
        s = scores_of(twice, qt[0])
        s0[at, :] = s
        return jnp.maximum(m, jnp.max(by_eight(s), axis=0))

    def partner_keys(g, m):
        def wait(n):
            arrival(kvr.at[1, GROUP * g + n], fw_ss.at[GROUP * g + n], fw_rs.at[GROUP * g + n]).wait_recv()

        loop(4, wait)
        return first_scores(1, g, m)

    m = jnp.full((8, TQ), -jnp.inf, f32)
    m = lax.fori_loop(0, 4, lambda g, m: first_scores(0, g, m), m)
    m = lax.fori_loop(0, 4, partner_keys, m)

    def two_tiles(p, carry):
        top, scale = carry

        @pl.when(jnp.logical_or(p == 2, jnp.logical_or(p == 4, p == 7)))
        def _():
            make_queries(lax.div(p, 2))

        m, total, out = attention_step(qt[2 * p + 1], top, scale, kk, vt, s1, s0)
        ot[jnp.maximum(2 * p - 1, 0)] = out
        top, scale = row_top(m), row_scale(total)

        @pl.when(p == 3)
        def _():
            w_arrival(1, wf.at[me.left])
            w_arrival(2, wf.at[me.right])
            for copy in w_next:
                copy.start()

        @pl.when(p == 8)
        def _():
            w_arrival(3, wf.at[me.opp, top_half])
            w_arrival(4, wf.at[me.opp, low_half])
            for copy in w_last:
                copy.start()

        m, total, out = attention_step(
            qt[jnp.minimum(2 * p + 2, TILES - 1)], top, scale, kk, vt, s0, s1
        )
        ot[2 * p] = out

        @pl.when(jnp.logical_or(p == 2, jnp.logical_or(p == 5, p == 7)))
        def _():
            send_back(lax.div(p, 3))

        return row_top(m), row_scale(total)

    _, scale = lax.fori_loop(
        0, TILES // 2, two_tiles, (row_top(m), jnp.zeros((1, TQ), f32))
    )
    _, _, out = attention_step(None, None, scale, kk, vt, s1, None, scores=False, exps=False)
    ot[TILES - 1] = out
    send_back(3)
    attr[me.head] = atts[me.own]

    def sent(n):
        @pl.when(n != me.own)
        def _():
            kv_copy(n).wait_send()
            q_copy(n).wait_send()

        fw_copy(n).wait_send()

    loop(16, sent)
    loop(12, lambda n: at_copy(n).wait_send())
    for copy in w_own + w_next + w_last:
        copy.wait_send()

    w_arrival(0, wf.at[me.sib])
    other = me.sib - me.dp
    w_arrival(5, wf.at[me.left + other])
    w_arrival(6, wf.at[me.right + other])
    w_arrival(7, wf.at[me.opp + other, top_half])
    w_arrival(8, wf.at[me.opp + other, low_half])
    own_w.wait()

    def heads_in(j):
        @pl.when(j != me.head)
        def _():
            arrival(attr.at[j], at_ss.at[j], at_rs.at[j]).wait_recv()

    loop(16, heads_in)

    def project(n):
        rows = jnp.concatenate([attr[j] for j in range(KV)], axis=1)
        product = lax.dot_general(rows, wf[n], (((1,), (0,)), ((), ())), preferred_element_type=f32)
        out_ref[0, :, pl.ds(pl.multiple_of(n * W_COLS, W_COLS), W_COLS)] = product.astype(bf16)

    loop(8, project)

    for n in range(12, 16):
        if n < 14:
            pl.when(n != me.own)(lambda n=n: at_copy(n).wait_send())
        else:
            at_copy(n).wait_send()


def on_device(queries, keys, values, q_gain, k_gain, w_out):
    dma = pltpu.SemaphoreType.DMA
    vmem = pl.BlockSpec(memory_space=pltpu.VMEM)
    anywhere = pl.BlockSpec(memory_space=pl.ANY)
    return pl.pallas_call(
        layer,
        out_shape=jax.ShapeDtypeStruct((1, TOK, W_ROWS), bf16),
        in_specs=[anywhere] * 4 + [vmem] * 2,
        out_specs=vmem,
        scratch_shapes=[
            pltpu.VMEM((16, TOK, 128), bf16),
            pltpu.VMEM((16, TOK, 128), bf16),
            pltpu.VMEM((2, 16, TOK, 128), bf16),
            pltpu.VMEM((16, TOK, 128), bf16),
            pltpu.VMEM((KEYS, 128), bf16),
            pltpu.VMEM((HD, KEYS), bf16),
            pltpu.VMEM((TILES, 2 * HD, TQ), bf16),
            pltpu.VMEM((KEYS, TQ), f32),
            pltpu.VMEM((KEYS, TQ), f32),
            pltpu.VMEM((TILES, HD, TQ), f32),
            pltpu.VMEM((16, TOK, 128), bf16),
            pltpu.VMEM((16, TOK, 128), bf16),
            pltpu.VMEM((8, W_ROWS, W_COLS), bf16),
            dma((16,)), dma((16,)), dma((16,)), dma((16,)),
            dma((16,)), dma((16,)), dma((16,)), dma((16,)),
            dma((9,)), dma((9,)), dma,
            pltpu.VMEM((TOK, KV * HD), bf16),
            pltpu.VMEM((TOK, KV * HD), bf16),
            pltpu.VMEM((TOK, QH * HD), bf16),
            dma((3,)),
        ],
        compiler_params=pltpu.CompilerParams(
            collective_id=0, has_side_effects=True, vmem_limit_bytes=60 * 2**20
        ),
    )(
        jnp.swapaxes(queries, 1, 2),
        jnp.swapaxes(keys, 1, 2),
        jnp.swapaxes(values, 1, 2),
        w_out,
        q_gain,
        k_gain,
    )


def solution(mesh):
    return jax.shard_map(
        on_device,
        mesh=mesh,
        in_specs=(P("dp", None, "sp"), P("dp", None, "sp"), P("dp", None, "sp"), P(), P(), P(None, "dp")),
        out_specs=P("dp", "sp", None),
        check_vma=False,
    )
```

```python
import jax
import jax.numpy as jnp
from jax import lax
from jax.experimental import pallas as pl
from jax.experimental.pallas import tpu as pltpu
from jax.sharding import PartitionSpec as P

HD = 64
QH = 32
KV = 16
GRID_W = 64
Z = 8
Y = 4
X = 4
TOK = 160
KEYS = 5120
TQ = 256
TILES = 20
KC = 256
GROUP = 4
SPAN = GROUP * TOK
W_ROWS = 2048
W_COLS = 256

epsilon = 1e-06
octaves = -13.287712379549449 / 16
log2_scale = HD ** (-0.5) * 1.4426950408889634
f32 = jnp.float32
bf16 = jnp.bfloat16
MESH = pl.DeviceIdType.MESH


def lanes(rows):
    return lax.broadcasted_iota(jnp.int32, (rows, 2 * HD), 1)


def rotary_tables(first_row):
    lane = lanes(TOK)
    position = first_row + lax.broadcasted_iota(jnp.int32, (TOK, 2 * HD), 0)
    place = jnp.where((lane & 32) == 0, position >> 6, position & (GRID_W - 1)).astype(f32)
    angle = place * jnp.exp2((lane & 15).astype(f32) * octaves)
    sin_table = jnp.sin(angle)
    return jnp.cos(angle), jnp.where((lane & 16) == 0, -sin_table, sin_table)


def head_sums():
    row = lax.broadcasted_iota(jnp.int32, (4 * HD, 2 * HD), 0)
    col = lax.broadcasted_iota(jnp.int32, (4 * HD, 2 * HD), 1)
    return jnp.where(((row >> 6) & 1) == (col >> 6), 1.0, 0.0).astype(bf16)


def turned(u, gain, tables, ones):
    square = u * u
    high = square.astype(bf16)
    low = (square - high.astype(f32)).astype(bf16)
    sums = lax.dot_general(
        jnp.concatenate([high, low], axis=1), ones, (((1,), (0,)), ((), ())), preferred_element_type=f32
    )
    n = u * lax.rsqrt(sums * (1.0 / HD) + epsilon) * gain
    rot = jnp.where(
        (lanes(TOK) & 16) == 0, pltpu.roll(n, 2 * HD - 16, 1), pltpu.roll(n, 16, 1)
    )
    return n * tables[0] + rot * tables[1]


def div(a, b):
    return a // b if isinstance(a, int) else lax.div(a, b)


def rem(a, b):
    return a % b if isinstance(a, int) else lax.rem(a, b)


class Place:
    def __init__(self):
        sp = lax.axis_index("sp")
        self.dp = lax.axis_index("dp")
        self.z, self.y = lax.div(sp, Y), lax.rem(sp, Y)
        self.g = lax.div(self.y, 2)
        self.e = self.g * (3 - self.y) + (1 - self.g) * self.y
        self.head = 2 * self.z + self.e
        self.own = 12 + self.e
        self.partner = self.z * Y + 3 - self.y
        x, self.c = lax.div(self.dp, 2), lax.rem(self.dp, 2)
        self.left = lax.rem(x + X - 1, X) * 2 + self.c
        self.right = lax.rem(x + 1, X) * 2 + self.c
        self.sib = self.dp + 1 - 2 * self.c
        self.opp = lax.rem(x + 2, X) * 2 + self.c

    def offset(self, n):
        i = rem(div(n, 2) + 2, Z)
        return div(i + 1, 2) * (2 * rem(i, 2) - 1)

    def at(self, z, e):
        return z * Y + self.g * 3 + e * (1 - 2 * self.g)

    def target_z(self, n):
        return lax.rem(self.z + self.offset(n) + Z, Z)

    def source_z(self, n):
        return lax.rem(self.z - self.offset(n) + Z, Z)

    def slot_there(self, n):
        return 2 * div(n, 2) + self.e


def all_slots(me, body):
    for n in range(16):
        if n in (12, 13):
            pl.when(n != me.own)(lambda n=n: body(n))
        else:
            body(n)


def loop(count, body):
    def step(n, carry):
        body(n)
        return carry

    lax.fori_loop(0, count, step, 0)


def scores_of(k, q):
    return lax.dot_general(k, q, (((1,), (0,)), ((), ())), preferred_element_type=f32)


def by_eight(x):
    return x.reshape(x.shape[0] // 8, 8, TQ)


def attention_step(q, top, scale, kk, vt, x_ref, y_ref, scores=True, exps=True):
    m = jnp.full((8, TQ), -jnp.inf, f32)
    total = jnp.zeros((8, TQ), f32)
    out = None
    tops = jnp.broadcast_to(top, (8, TQ)) if exps else None
    scales = jnp.broadcast_to(scale, (8, TQ))
    zeros = []
    for j in range(KEYS // KC):
        at = slice(j * KC, (j + 1) * KC)
        if exps:
            e = jnp.exp2(by_eight(y_ref[at, :]) - tops)
            y_ref[at, :] = e.reshape(KC, TQ)
            part = jnp.sum(e, axis=0)
            total = total + part
            zeros.append(jnp.minimum(part, 0.0))
        by = scales + zeros[j - 2] if exps and j >= 2 else scales
        weights = (by_eight(x_ref[at, :]) * by).reshape(KC, TQ).astype(bf16)
        part = lax.dot_general(vt[:, at], weights, (((1,), (0,)), ((), ())), preferred_element_type=f32)
        out = part if out is None else out + part
        if scores:
            s = scores_of(kk[at, :], q)
            x_ref[at, :] = s
            m = jnp.maximum(m, jnp.max(by_eight(s), axis=0))
    return m, total, out


def layer(
    q_ref, k_ref, v_ref, w_ref, qg_ref, kg_ref, out_ref,
    kvs, qs, kvr, qr, kk, vt, qt, s0, s1, ot, atts, attr, wf,
    kv_ss, kv_rs, fw_ss, fw_rs, q_ss, q_rs, at_ss, at_rs, w_ss, w_rs, own_sem,
    k_in, v_in, q_in, in_sem,
):
    me = Place()

    def remote(src, dst, ss, rs, **device):
        return pltpu.make_async_remote_copy(
            src_ref=src, dst_ref=dst, send_sem=ss, recv_sem=rs, device_id=device, device_id_type=MESH
        )

    barrier = pltpu.get_barrier_semaphore()

    def hello(**device):
        pl.semaphore_signal(barrier, inc=1, device_id=device, device_id_type=MESH)

    inputs = [
        pltpu.make_async_copy(src.at[0], dst, in_sem.at[n])
        for n, (src, dst) in enumerate(((k_ref, k_in), (v_ref, v_in), (q_ref, q_in)))
    ]
    for copy in inputs:
        copy.start()
    all_slots(me, lambda n: hello(sp=me.at(me.target_z(n), rem(n, 2))))
    hello(sp=me.partner)
    hello(dp=me.sib)
    hello(dp=me.left)
    hello(dp=me.right)

    tables = rotary_tables(lax.axis_index("sp") * TOK)
    ones = head_sums()

    def two_heads(ref):
        gain = ref[...].reshape(1, HD)
        return jnp.concatenate([gain, gain], axis=1)

    q_gain, k_gain = two_heads(qg_ref), two_heads(kg_ref)
    first_head = lanes(TOK) < HD

    def make_kv(i):
        at = pl.ds(pl.multiple_of(me.target_z(2 * i) * 2 * HD, 2 * HD), 2 * HD)
        k = turned(k_in[:, at].astype(f32), k_gain, tables, ones)
        v = v_in[:, at].astype(f32)
        kvs[2 * i] = jnp.where(first_head, k, pltpu.roll(v, HD, 1)).astype(bf16)
        kvs[2 * i + 1] = jnp.where(first_head, pltpu.roll(k, HD, 1), v).astype(bf16)

    def make_q(n):
        j = 2 * me.target_z(n) + rem(n, 2)
        at = pl.ds(pl.multiple_of(j * 2 * HD, 2 * HD), 2 * HD)
        qs[n] = turned(q_in[:, at].astype(f32), q_gain, tables, ones).astype(bf16)

    def kv_copy(n):
        there = me.slot_there(n)
        return remote(
            kvs.at[n], kvr.at[0, there], kv_ss.at[n], kv_rs.at[there],
            sp=me.at(me.target_z(n), rem(n, 2)),
        )

    def q_copy(n):
        there = me.slot_there(n)
        return remote(
            qs.at[n], qr.at[there], q_ss.at[n], q_rs.at[there],
            sp=me.at(me.target_z(n), rem(n, 2)),
        )

    def fw_copy(n):
        return remote(kvr.at[0, n], kvr.at[1, n], fw_ss.at[n], fw_rs.at[n], sp=me.partner)

    def at_copy(n):
        return remote(
            atts.at[n], attr.at[me.head], at_ss.at[n], at_rs.at[me.head],
            sp=me.at(me.source_z(n), rem(n, 2)),
        )

    def arrival(ref, ss, rs):
        return remote(ref, ref, ss, rs, sp=me.partner)

    top_half, low_half = pl.ds(0, W_ROWS // 2), pl.ds(W_ROWS // 2, W_ROWS // 2)

    def w_copy(kind, src, dst, dp):
        return remote(src, dst, w_ss.at[kind], w_rs.at[kind], dp=dp)

    w_own = (
        w_copy(0, w_ref, wf.at[me.dp], me.sib),
        w_copy(1, w_ref, wf.at[me.dp], me.right),
        w_copy(2, w_ref, wf.at[me.dp], me.left),
    )
    w_next = (
        w_copy(3, wf.at[me.left, top_half], wf.at[me.left, top_half], me.right),
        w_copy(4, wf.at[me.right, low_half], wf.at[me.right, low_half], me.left),
        w_copy(5, wf.at[me.left], wf.at[me.left], me.sib),
        w_copy(6, wf.at[me.right], wf.at[me.right], me.sib),
    )
    w_last = (
        w_copy(7, wf.at[me.opp, top_half], wf.at[me.opp, top_half], me.sib),
        w_copy(8, wf.at[me.opp, low_half], wf.at[me.opp, low_half], me.sib),
    )

    def w_arrival(kind, ref):
        arrival(ref, w_ss.at[kind], w_rs.at[kind]).wait_recv()

    def make_four(r):
        make_kv(2 * r)
        make_kv(2 * r + 1)

    inputs[0].wait()
    inputs[1].wait()
    loop(4, make_four)
    pl.semaphore_wait(barrier, 19)

    all_slots(me, lambda n: kv_copy(n).start())
    kvr[0, me.own] = kvs[me.own]

    def make_q_four(r):
        for n in range(4):
            make_q(4 * r + n)

    inputs[2].wait()
    loop(4, make_q_four)

    all_slots(me, lambda n: q_copy(n).start())
    qr[me.own] = qs[me.own]
    own_w = pltpu.make_async_copy(w_ref, wf.at[me.dp], own_sem)
    own_w.start()
    for copy in w_own:
        copy.start()

    def forward(n):
        @pl.when(n != me.own)
        def _():
            arrival(kvr.at[0, n], kv_ss.at[n], kv_rs.at[n]).wait_recv()

        fw_copy(n).start()


    def make_keys(half, g):
        block = kvr[half, pl.ds(GROUP * g, GROUP)].reshape(SPAN, 2 * HD)
        at = pl.ds(pl.multiple_of((half * GROUP + g) * SPAN, 128), SPAN)
        twice = jnp.concatenate([block[:, :HD], block[:, :HD]], axis=1)
        kk[at, :] = twice
        vt[:, at] = jnp.transpose(block)[HD:]

    def make_queries(g):
        def wait(r):
            n = GROUP * g + r

            @pl.when(n != me.own)
            def _():
                arrival(qr.at[n], q_ss.at[n], q_rs.at[n]).wait_recv()

        loop(4, wait)
        block = qr[pl.ds(GROUP * g, GROUP)].reshape(SPAN, 2 * HD)
        t = jnp.transpose(block.astype(f32)) * log2_scale
        t = jnp.concatenate([t[:HD], t[HD:]], axis=1)
        first = t.astype(bf16)
        second = (t - first.astype(f32)).astype(bf16)
        terms = jnp.concatenate([first, second], axis=0)
        for u in range(5):
            qt[5 * g + u] = terms[:, u * TQ : (u + 1) * TQ]

    def send_back(g):
        tiles = jnp.concatenate([ot[5 * g + u] for u in range(5)], axis=1)
        heads = jnp.concatenate([tiles[:, :SPAN], tiles[:, SPAN:]], axis=0)
        atts[pl.ds(GROUP * g, GROUP)] = jnp.transpose(heads).astype(bf16).reshape(GROUP, TOK, 2 * HD)

        def send(r):
            n = GROUP * g + r

            @pl.when(n != me.own)
            def _():
                at_copy(n).start()

        loop(4, send)

    row_top = lambda m: jnp.max(m, axis=0, keepdims=True)
    row_scale = lambda total: 1.0 / jnp.sum(total, axis=0, keepdims=True)
    s1[...] = jnp.zeros_like(s1)

    def own_keys(g):
        loop(GROUP, lambda r: forward(GROUP * g + r))
        make_keys(0, g)

    loop(4, own_keys)
    make_queries(0)

    def first_scores(half, g, m):
        at = pl.ds(pl.multiple_of((half * GROUP + g) * SPAN, 128), SPAN)
        s = scores_of(kk[at, :], qt[0])
        s0[at, :] = s
        return jnp.maximum(m, jnp.max(by_eight(s), axis=0))

    def partner_keys(g, m):
        def wait(n):
            arrival(kvr.at[1, GROUP * g + n], fw_ss.at[GROUP * g + n], fw_rs.at[GROUP * g + n]).wait_recv()

        loop(4, wait)
        make_keys(1, g)
        return first_scores(1, g, m)

    m = jnp.full((8, TQ), -jnp.inf, f32)
    m = lax.fori_loop(0, 4, lambda g, m: first_scores(0, g, m), m)
    m = lax.fori_loop(0, 4, partner_keys, m)

    def two_tiles(p, carry):
        top, scale = carry

        @pl.when(jnp.logical_or(p == 2, jnp.logical_or(p == 4, p == 7)))
        def _():
            make_queries(lax.div(p, 2))

        m, total, out = attention_step(qt[2 * p + 1], top, scale, kk, vt, s1, s0)
        ot[jnp.maximum(2 * p - 1, 0)] = out
        top, scale = row_top(m), row_scale(total)

        @pl.when(p == 3)
        def _():
            w_arrival(1, wf.at[me.left])
            w_arrival(2, wf.at[me.right])
            for copy in w_next:
                copy.start()

        @pl.when(p == 8)
        def _():
            w_arrival(3, wf.at[me.opp, top_half])
            w_arrival(4, wf.at[me.opp, low_half])
            for copy in w_last:
                copy.start()

        m, total, out = attention_step(
            qt[jnp.minimum(2 * p + 2, TILES - 1)], top, scale, kk, vt, s0, s1
        )
        ot[2 * p] = out

        @pl.when(jnp.logical_or(p == 2, jnp.logical_or(p == 5, p == 7)))
        def _():
            send_back(lax.div(p, 3))

        return row_top(m), row_scale(total)

    _, scale = lax.fori_loop(
        0, TILES // 2, two_tiles, (row_top(m), jnp.zeros((1, TQ), f32))
    )
    _, _, out = attention_step(None, None, scale, kk, vt, s1, None, scores=False, exps=False)
    ot[TILES - 1] = out
    send_back(3)
    attr[me.head] = atts[me.own]

    def sent(n):
        @pl.when(n != me.own)
        def _():
            kv_copy(n).wait_send()
            q_copy(n).wait_send()

        fw_copy(n).wait_send()

    loop(16, sent)
    loop(12, lambda n: at_copy(n).wait_send())
    for copy in w_own + w_next + w_last:
        copy.wait_send()

    w_arrival(0, wf.at[me.sib])
    other = me.sib - me.dp
    w_arrival(5, wf.at[me.left + other])
    w_arrival(6, wf.at[me.right + other])
    w_arrival(7, wf.at[me.opp + other, top_half])
    w_arrival(8, wf.at[me.opp + other, low_half])
    own_w.wait()

    def heads_in(j):
        @pl.when(j != me.head)
        def _():
            arrival(attr.at[j], at_ss.at[j], at_rs.at[j]).wait_recv()

    loop(16, heads_in)

    def project(n):
        rows = jnp.concatenate([attr[j] for j in range(KV)], axis=1)
        product = lax.dot_general(rows, wf[n], (((1,), (0,)), ((), ())), preferred_element_type=f32)
        out_ref[0, :, pl.ds(pl.multiple_of(n * W_COLS, W_COLS), W_COLS)] = product.astype(bf16)

    loop(8, project)

    for n in range(12, 16):
        if n < 14:
            pl.when(n != me.own)(lambda n=n: at_copy(n).wait_send())
        else:
            at_copy(n).wait_send()


def on_device(queries, keys, values, q_gain, k_gain, w_out):
    dma = pltpu.SemaphoreType.DMA
    vmem = pl.BlockSpec(memory_space=pltpu.VMEM)
    anywhere = pl.BlockSpec(memory_space=pl.ANY)
    return pl.pallas_call(
        layer,
        out_shape=jax.ShapeDtypeStruct((1, TOK, W_ROWS), bf16),
        in_specs=[anywhere] * 4 + [vmem] * 2,
        out_specs=vmem,
        scratch_shapes=[
            pltpu.VMEM((16, TOK, 128), bf16),
            pltpu.VMEM((16, TOK, 128), bf16),
            pltpu.VMEM((2, 16, TOK, 128), bf16),
            pltpu.VMEM((16, TOK, 128), bf16),
            pltpu.VMEM((KEYS, 128), bf16),
            pltpu.VMEM((HD, KEYS), bf16),
            pltpu.VMEM((TILES, 2 * HD, TQ), bf16),
            pltpu.VMEM((KEYS, TQ), f32),
            pltpu.VMEM((KEYS, TQ), f32),
            pltpu.VMEM((TILES, HD, TQ), f32),
            pltpu.VMEM((16, TOK, 128), bf16),
            pltpu.VMEM((16, TOK, 128), bf16),
            pltpu.VMEM((8, W_ROWS, W_COLS), bf16),
            dma((16,)), dma((16,)), dma((16,)), dma((16,)),
            dma((16,)), dma((16,)), dma((16,)), dma((16,)),
            dma((9,)), dma((9,)), dma,
            pltpu.VMEM((TOK, KV * HD), bf16),
            pltpu.VMEM((TOK, KV * HD), bf16),
            pltpu.VMEM((TOK, QH * HD), bf16),
            dma((3,)),
        ],
        compiler_params=pltpu.CompilerParams(
            collective_id=0, has_side_effects=True, vmem_limit_bytes=60 * 2**20
        ),
    )(
        jnp.swapaxes(queries, 1, 2),
        jnp.swapaxes(keys, 1, 2),
        jnp.swapaxes(values, 1, 2),
        w_out,
        q_gain,
        k_gain,
    )


def solution(mesh):
    return jax.shard_map(
        on_device,
        mesh=mesh,
        in_specs=(P("dp", None, "sp"), P("dp", None, "sp"), P("dp", None, "sp"), P(), P(), P(None, "dp")),
        out_specs=P("dp", "sp", None),
        check_vma=False,
    )
```

```python
import jax
import jax.numpy as jnp
from jax import lax
from jax.experimental import pallas as pl
from jax.experimental.pallas import tpu as pltpu
from jax.sharding import PartitionSpec as P

HD = 64
QH = 32
KV = 16
GRID_W = 64
Z = 8
Y = 4
X = 4
TOK = 160
KEYS = 5120
TQ = 256
TILES = 20
KC = 256
GROUP = 4
SPAN = GROUP * TOK
W_ROWS = 2048
W_COLS = 256

epsilon = 1e-06
octaves = -13.287712379549449 / 16
log2_scale = HD ** (-0.5) * 1.4426950408889634
f32 = jnp.float32
bf16 = jnp.bfloat16
MESH = pl.DeviceIdType.MESH


def lanes(rows):
    return lax.broadcasted_iota(jnp.int32, (rows, 2 * HD), 1)


def rotary_tables(first_row):
    lane = lanes(TOK)
    position = first_row + lax.broadcasted_iota(jnp.int32, (TOK, 2 * HD), 0)
    place = jnp.where((lane & 32) == 0, position >> 6, position & (GRID_W - 1)).astype(f32)
    angle = place * jnp.exp2((lane & 15).astype(f32) * octaves)
    sin_table = jnp.sin(angle)
    return jnp.cos(angle), jnp.where((lane & 16) == 0, -sin_table, sin_table)


def head_sums():
    row = lax.broadcasted_iota(jnp.int32, (4 * HD, 2 * HD), 0)
    col = lax.broadcasted_iota(jnp.int32, (4 * HD, 2 * HD), 1)
    return jnp.where(((row >> 6) & 1) == (col >> 6), 1.0, 0.0).astype(bf16)


def turned(u, gain, tables, ones):
    square = u * u
    high = square.astype(bf16)
    low = (square - high.astype(f32)).astype(bf16)
    sums = lax.dot_general(
        jnp.concatenate([high, low], axis=1), ones, (((1,), (0,)), ((), ())), preferred_element_type=f32
    )
    n = u * lax.rsqrt(sums * (1.0 / HD) + epsilon) * gain
    rot = jnp.where(
        (lanes(TOK) & 16) == 0, pltpu.roll(n, 2 * HD - 16, 1), pltpu.roll(n, 16, 1)
    )
    return n * tables[0] + rot * tables[1]


def div(a, b):
    return a // b if isinstance(a, int) else lax.div(a, b)


def rem(a, b):
    return a % b if isinstance(a, int) else lax.rem(a, b)


class Place:
    def __init__(self):
        sp = lax.axis_index("sp")
        self.dp = lax.axis_index("dp")
        self.z, self.y = lax.div(sp, Y), lax.rem(sp, Y)
        self.g = lax.div(self.y, 2)
        self.e = self.g * (3 - self.y) + (1 - self.g) * self.y
        self.head = 2 * self.z + self.e
        self.own = 12 + self.e
        self.partner = self.z * Y + 3 - self.y
        x, self.c = lax.div(self.dp, 2), lax.rem(self.dp, 2)
        self.left = lax.rem(x + X - 1, X) * 2 + self.c
        self.right = lax.rem(x + 1, X) * 2 + self.c
        self.sib = self.dp + 1 - 2 * self.c
        self.opp = lax.rem(x + 2, X) * 2 + self.c

    def offset(self, n):
        i = rem(div(n, 2) + 2, Z)
        return div(i + 1, 2) * (2 * rem(i, 2) - 1)

    def at(self, z, e):
        return z * Y + self.g * 3 + e * (1 - 2 * self.g)

    def target_z(self, n):
        return lax.rem(self.z + self.offset(n) + Z, Z)

    def source_z(self, n):
        return lax.rem(self.z - self.offset(n) + Z, Z)

    def slot_there(self, n):
        return 2 * div(n, 2) + self.e


def all_slots(me, body, first=0):
    for n in [(first + n) % 16 for n in range(16)]:
        if n in (12, 13):
            pl.when(n != me.own)(lambda n=n: body(n))
        else:
            body(n)


def loop(count, body):
    def step(n, carry):
        body(n)
        return carry

    lax.fori_loop(0, count, step, 0)


def scores_of(k, q):
    return lax.dot_general(k, q, (((1,), (0,)), ((), ())), preferred_element_type=f32)


def by_eight(x):
    return x.reshape(x.shape[0] // 8, 8, TQ)


def attention_step(q, top, scale, kk, vt, x_ref, y_ref, scores=True, exps=True):
    m = jnp.full((8, TQ), -jnp.inf, f32)
    total = jnp.zeros((8, TQ), f32)
    out = None
    tops = jnp.broadcast_to(top, (8, TQ)) if exps else None
    scales = jnp.broadcast_to(scale, (8, TQ))
    zeros = []
    for j in range(KEYS // KC):
        at = slice(j * KC, (j + 1) * KC)
        if exps:
            e = jnp.exp2(by_eight(y_ref[at, :]) - tops)
            y_ref[at, :] = e.reshape(KC, TQ)
            part = jnp.sum(e, axis=0)
            total = total + part
            zeros.append(jnp.minimum(part, 0.0))
        by = scales + zeros[j - 2] if exps and j >= 2 else scales
        weights = (by_eight(x_ref[at, :]) * by).reshape(KC, TQ).astype(bf16)
        part = lax.dot_general(vt[:, at], weights, (((1,), (0,)), ((), ())), preferred_element_type=f32)
        out = part if out is None else out + part
        if scores:
            s = scores_of(kk[at, :], q)
            x_ref[at, :] = s
            m = jnp.maximum(m, jnp.max(by_eight(s), axis=0))
    return m, total, out


def layer(
    q_ref, k_ref, v_ref, w_ref, qg_ref, kg_ref, out_ref,
    kvs, qs, kvr, qr, kk, vt, qt, s0, s1, ot, atts, attr, wf,
    kv_ss, kv_rs, fw_ss, fw_rs, q_ss, q_rs, at_ss, at_rs, w_ss, w_rs, own_sem,
    k_in, v_in, q_in, in_sem,
):
    me = Place()

    def remote(src, dst, ss, rs, **device):
        return pltpu.make_async_remote_copy(
            src_ref=src, dst_ref=dst, send_sem=ss, recv_sem=rs, device_id=device, device_id_type=MESH
        )

    barrier = pltpu.get_barrier_semaphore()

    def hello(**device):
        pl.semaphore_signal(barrier, inc=1, device_id=device, device_id_type=MESH)

    inputs = [
        pltpu.make_async_copy(src.at[0], dst, in_sem.at[n])
        for n, (src, dst) in enumerate(((k_ref, k_in), (v_ref, v_in), (q_ref, q_in)))
    ]
    for copy in inputs:
        copy.start()
    all_slots(me, lambda n: hello(sp=me.at(me.target_z(n), rem(n, 2))))
    hello(sp=me.partner)
    hello(dp=me.sib)
    hello(dp=me.left)
    hello(dp=me.right)

    tables = rotary_tables(lax.axis_index("sp") * TOK)
    ones = head_sums()

    def two_heads(ref):
        gain = ref[...].reshape(1, HD)
        return jnp.concatenate([gain, gain], axis=1)

    q_gain, k_gain = two_heads(qg_ref), two_heads(kg_ref)
    first_head = lanes(TOK) < HD

    def make_kv(i):
        at = pl.ds(pl.multiple_of(me.target_z(2 * i) * 2 * HD, 2 * HD), 2 * HD)
        k = turned(k_in[:, at].astype(f32), k_gain, tables, ones)
        v = v_in[:, at].astype(f32)
        kvs[2 * i] = jnp.where(first_head, k, pltpu.roll(v, HD, 1)).astype(bf16)
        kvs[2 * i + 1] = jnp.where(first_head, pltpu.roll(k, HD, 1), v).astype(bf16)

    def make_q(n):
        j = 2 * me.target_z(n) + rem(n, 2)
        at = pl.ds(pl.multiple_of(j * 2 * HD, 2 * HD), 2 * HD)
        qs[n] = turned(q_in[:, at].astype(f32), q_gain, tables, ones).astype(bf16)

    def kv_copy(n):
        there = me.slot_there(n)
        return remote(
            kvs.at[n], kvr.at[0, there], kv_ss.at[n], kv_rs.at[there],
            sp=me.at(me.target_z(n), rem(n, 2)),
        )

    def q_copy(n):
        there = me.slot_there(n)
        return remote(
            qs.at[n], qr.at[there], q_ss.at[n], q_rs.at[there],
            sp=me.at(me.target_z(n), rem(n, 2)),
        )

    def fw_copy(n):
        return remote(kvr.at[0, n], kvr.at[1, n], fw_ss.at[n], fw_rs.at[n], sp=me.partner)

    def at_copy(n):
        return remote(
            atts.at[n], attr.at[me.head], at_ss.at[n], at_rs.at[me.head],
            sp=me.at(me.source_z(n), rem(n, 2)),
        )

    def arrival(ref, ss, rs):
        return remote(ref, ref, ss, rs, sp=me.partner)

    top_half, low_half = pl.ds(0, W_ROWS // 2), pl.ds(W_ROWS // 2, W_ROWS // 2)

    def w_copy(kind, src, dst, dp):
        return remote(src, dst, w_ss.at[kind], w_rs.at[kind], dp=dp)

    w_own = (
        w_copy(0, w_ref, wf.at[me.dp], me.sib),
        w_copy(1, w_ref, wf.at[me.dp], me.right),
        w_copy(2, w_ref, wf.at[me.dp], me.left),
    )
    w_next = (
        w_copy(3, wf.at[me.left, top_half], wf.at[me.left, top_half], me.right),
        w_copy(4, wf.at[me.right, low_half], wf.at[me.right, low_half], me.left),
        w_copy(5, wf.at[me.left], wf.at[me.left], me.sib),
        w_copy(6, wf.at[me.right], wf.at[me.right], me.sib),
    )
    w_last = (
        w_copy(7, wf.at[me.opp, top_half], wf.at[me.opp, top_half], me.sib),
        w_copy(8, wf.at[me.opp, low_half], wf.at[me.opp, low_half], me.sib),
    )

    def w_arrival(kind, ref):
        arrival(ref, w_ss.at[kind], w_rs.at[kind]).wait_recv()

    def make_four(r):
        make_kv(2 * r)
        make_kv(2 * r + 1)

    inputs[0].wait()
    inputs[1].wait()
    loop(4, make_four)
    pl.semaphore_wait(barrier, 19)

    all_slots(me, lambda n: kv_copy(n).start(), first=12)
    kvr[0, me.own] = kvs[me.own]

    def make_q_four(r):
        for n in range(4):
            make_q(4 * r + n)

    inputs[2].wait()
    loop(4, make_q_four)

    all_slots(me, lambda n: q_copy(n).start())
    qr[me.own] = qs[me.own]
    own_w = pltpu.make_async_copy(w_ref, wf.at[me.dp], own_sem)
    own_w.start()
    for copy in w_own:
        copy.start()

    def forward(n):
        @pl.when(n != me.own)
        def _():
            arrival(kvr.at[0, n], kv_ss.at[n], kv_rs.at[n]).wait_recv()

        fw_copy(n).start()


    def make_keys(half, g):
        block = kvr[half, pl.ds(GROUP * g, GROUP)].reshape(SPAN, 2 * HD)
        at = pl.ds(pl.multiple_of((half * GROUP + g) * SPAN, 128), SPAN)
        twice = jnp.concatenate([block[:, :HD], block[:, :HD]], axis=1)
        kk[at, :] = twice
        vt[:, at] = jnp.transpose(block)[HD:]

    def make_queries(g):
        def wait(r):
            n = GROUP * g + r

            @pl.when(n != me.own)
            def _():
                arrival(qr.at[n], q_ss.at[n], q_rs.at[n]).wait_recv()

        loop(4, wait)
        block = qr[pl.ds(GROUP * g, GROUP)].reshape(SPAN, 2 * HD)
        t = jnp.transpose(block.astype(f32)) * log2_scale
        t = jnp.concatenate([t[:HD], t[HD:]], axis=1)
        first = t.astype(bf16)
        second = (t - first.astype(f32)).astype(bf16)
        terms = jnp.concatenate([first, second], axis=0)
        for u in range(5):
            qt[5 * g + u] = terms[:, u * TQ : (u + 1) * TQ]

    def send_back(g):
        tiles = jnp.concatenate([ot[5 * g + u] for u in range(5)], axis=1)
        heads = jnp.concatenate([tiles[:, :SPAN], tiles[:, SPAN:]], axis=0)
        atts[pl.ds(GROUP * g, GROUP)] = jnp.transpose(heads).astype(bf16).reshape(GROUP, TOK, 2 * HD)

        def send(r):
            n = GROUP * g + r

            @pl.when(n != me.own)
            def _():
                at_copy(n).start()

        loop(4, send)

    row_top = lambda m: jnp.max(m, axis=0, keepdims=True)
    row_scale = lambda total: 1.0 / jnp.sum(total, axis=0, keepdims=True)
    s1[...] = jnp.zeros_like(s1)

    def own_keys(r):
        g = lax.rem(r + 3, 4)
        loop(GROUP, lambda r: forward(GROUP * g + r))
        make_keys(0, g)

    loop(4, own_keys)
    make_queries(0)

    def first_scores(half, g, m):
        at = pl.ds(pl.multiple_of((half * GROUP + g) * SPAN, 128), SPAN)
        s = scores_of(kk[at, :], qt[0])
        s0[at, :] = s
        return jnp.maximum(m, jnp.max(by_eight(s), axis=0))

    def partner_keys(r, m):
        g = lax.rem(r + 3, 4)

        def wait(n):
            arrival(kvr.at[1, GROUP * g + n], fw_ss.at[GROUP * g + n], fw_rs.at[GROUP * g + n]).wait_recv()

        loop(4, wait)
        make_keys(1, g)
        return first_scores(1, g, m)

    m = jnp.full((8, TQ), -jnp.inf, f32)
    m = lax.fori_loop(0, 4, lambda g, m: first_scores(0, g, m), m)
    m = lax.fori_loop(0, 4, partner_keys, m)

    def two_tiles(p, carry):
        top, scale = carry

        @pl.when(jnp.logical_or(p == 2, jnp.logical_or(p == 4, p == 7)))
        def _():
            make_queries(lax.div(p, 2))

        m, total, out = attention_step(qt[2 * p + 1], top, scale, kk, vt, s1, s0)
        ot[jnp.maximum(2 * p - 1, 0)] = out
        top, scale = row_top(m), row_scale(total)

        @pl.when(p == 3)
        def _():
            w_arrival(1, wf.at[me.left])
            w_arrival(2, wf.at[me.right])
            for copy in w_next:
                copy.start()

        @pl.when(p == 8)
        def _():
            w_arrival(3, wf.at[me.opp, top_half])
            w_arrival(4, wf.at[me.opp, low_half])
            for copy in w_last:
                copy.start()

        m, total, out = attention_step(
            qt[jnp.minimum(2 * p + 2, TILES - 1)], top, scale, kk, vt, s0, s1
        )
        ot[2 * p] = out

        @pl.when(jnp.logical_or(p == 2, jnp.logical_or(p == 5, p == 7)))
        def _():
            send_back(lax.div(p, 3))

        return row_top(m), row_scale(total)

    _, scale = lax.fori_loop(
        0, TILES // 2, two_tiles, (row_top(m), jnp.zeros((1, TQ), f32))
    )
    _, _, out = attention_step(None, None, scale, kk, vt, s1, None, scores=False, exps=False)
    ot[TILES - 1] = out
    send_back(3)
    attr[me.head] = atts[me.own]

    def sent(n):
        @pl.when(n != me.own)
        def _():
            kv_copy(n).wait_send()
            q_copy(n).wait_send()

        fw_copy(n).wait_send()

    loop(16, sent)
    loop(12, lambda n: at_copy(n).wait_send())
    for copy in w_own + w_next + w_last:
        copy.wait_send()

    w_arrival(0, wf.at[me.sib])
    other = me.sib - me.dp
    w_arrival(5, wf.at[me.left + other])
    w_arrival(6, wf.at[me.right + other])
    w_arrival(7, wf.at[me.opp + other, top_half])
    w_arrival(8, wf.at[me.opp + other, low_half])
    own_w.wait()

    def heads_in(j):
        @pl.when(j != me.head)
        def _():
            arrival(attr.at[j], at_ss.at[j], at_rs.at[j]).wait_recv()

    loop(16, heads_in)

    def project(n):
        rows = jnp.concatenate([attr[j] for j in range(KV)], axis=1)
        product = lax.dot_general(rows, wf[n], (((1,), (0,)), ((), ())), preferred_element_type=f32)
        out_ref[0, :, pl.ds(pl.multiple_of(n * W_COLS, W_COLS), W_COLS)] = product.astype(bf16)

    loop(8, project)

    for n in range(12, 16):
        if n < 14:
            pl.when(n != me.own)(lambda n=n: at_copy(n).wait_send())
        else:
            at_copy(n).wait_send()


def on_device(queries, keys, values, q_gain, k_gain, w_out):
    dma = pltpu.SemaphoreType.DMA
    vmem = pl.BlockSpec(memory_space=pltpu.VMEM)
    anywhere = pl.BlockSpec(memory_space=pl.ANY)
    return pl.pallas_call(
        layer,
        out_shape=jax.ShapeDtypeStruct((1, TOK, W_ROWS), bf16),
        in_specs=[anywhere] * 4 + [vmem] * 2,
        out_specs=vmem,
        scratch_shapes=[
            pltpu.VMEM((16, TOK, 128), bf16),
            pltpu.VMEM((16, TOK, 128), bf16),
            pltpu.VMEM((2, 16, TOK, 128), bf16),
            pltpu.VMEM((16, TOK, 128), bf16),
            pltpu.VMEM((KEYS, 128), bf16),
            pltpu.VMEM((HD, KEYS), bf16),
            pltpu.VMEM((TILES, 2 * HD, TQ), bf16),
            pltpu.VMEM((KEYS, TQ), f32),
            pltpu.VMEM((KEYS, TQ), f32),
            pltpu.VMEM((TILES, HD, TQ), f32),
            pltpu.VMEM((16, TOK, 128), bf16),
            pltpu.VMEM((16, TOK, 128), bf16),
            pltpu.VMEM((8, W_ROWS, W_COLS), bf16),
            dma((16,)), dma((16,)), dma((16,)), dma((16,)),
            dma((16,)), dma((16,)), dma((16,)), dma((16,)),
            dma((9,)), dma((9,)), dma,
            pltpu.VMEM((TOK, KV * HD), bf16),
            pltpu.VMEM((TOK, KV * HD), bf16),
            pltpu.VMEM((TOK, QH * HD), bf16),
            dma((3,)),
        ],
        compiler_params=pltpu.CompilerParams(
            collective_id=0, has_side_effects=True, vmem_limit_bytes=60 * 2**20
        ),
    )(
        jnp.swapaxes(queries, 1, 2),
        jnp.swapaxes(keys, 1, 2),
        jnp.swapaxes(values, 1, 2),
        w_out,
        q_gain,
        k_gain,
    )


def solution(mesh):
    return jax.shard_map(
        on_device,
        mesh=mesh,
        in_specs=(P("dp", None, "sp"), P("dp", None, "sp"), P("dp", None, "sp"), P(), P(), P(None, "dp")),
        out_specs=P("dp", "sp", None),
        check_vma=False,
    )
```

```python
import jax
import jax.numpy as jnp
from jax import lax
from jax.experimental import pallas as pl
from jax.experimental.pallas import tpu as pltpu
from jax.sharding import PartitionSpec as P

HD = 64
QH = 32
KV = 16
GRID_W = 64
Z = 8
Y = 4
X = 4
TOK = 160
KEYS = 5120
TQ = 256
TILES = 20
KC = 256
GROUP = 4
SPAN = GROUP * TOK
W_ROWS = 2048
W_COLS = 256

epsilon = 1e-06
octaves = -13.287712379549449 / 16
log2_scale = HD ** (-0.5) * 1.4426950408889634
f32 = jnp.float32
bf16 = jnp.bfloat16
MESH = pl.DeviceIdType.MESH


def lanes(rows):
    return lax.broadcasted_iota(jnp.int32, (rows, 2 * HD), 1)


def rotary_tables(first_row):
    lane = lanes(TOK)
    position = first_row + lax.broadcasted_iota(jnp.int32, (TOK, 2 * HD), 0)
    place = jnp.where((lane & 32) == 0, position >> 6, position & (GRID_W - 1)).astype(f32)
    angle = place * jnp.exp2((lane & 15).astype(f32) * octaves)
    sin_table = jnp.sin(angle)
    return jnp.cos(angle), jnp.where((lane & 16) == 0, -sin_table, sin_table)


def head_sums():
    row = lax.broadcasted_iota(jnp.int32, (4 * HD, 2 * HD), 0)
    col = lax.broadcasted_iota(jnp.int32, (4 * HD, 2 * HD), 1)
    return jnp.where(((row >> 6) & 1) == (col >> 6), 1.0, 0.0).astype(bf16)


def turned(u, gain, tables, ones):
    square = u * u
    high = square.astype(bf16)
    low = (square - high.astype(f32)).astype(bf16)
    sums = lax.dot_general(
        jnp.concatenate([high, low], axis=1), ones, (((1,), (0,)), ((), ())), preferred_element_type=f32
    )
    n = u * lax.rsqrt(sums * (1.0 / HD) + epsilon) * gain
    rot = jnp.where(
        (lanes(TOK) & 16) == 0, pltpu.roll(n, 2 * HD - 16, 1), pltpu.roll(n, 16, 1)
    )
    return n * tables[0] + rot * tables[1]


def div(a, b):
    return a // b if isinstance(a, int) else lax.div(a, b)


def rem(a, b):
    return a % b if isinstance(a, int) else lax.rem(a, b)


class Place:
    def __init__(self):
        sp = lax.axis_index("sp")
        self.dp = lax.axis_index("dp")
        self.z, self.y = lax.div(sp, Y), lax.rem(sp, Y)
        self.g = lax.div(self.y, 2)
        self.e = self.g * (3 - self.y) + (1 - self.g) * self.y
        self.head = 2 * self.z + self.e
        self.own = 12 + self.e
        self.partner = self.z * Y + 3 - self.y
        x, self.c = lax.div(self.dp, 2), lax.rem(self.dp, 2)
        self.left = lax.rem(x + X - 1, X) * 2 + self.c
        self.right = lax.rem(x + 1, X) * 2 + self.c
        self.sib = self.dp + 1 - 2 * self.c
        self.opp = lax.rem(x + 2, X) * 2 + self.c

    def offset(self, n):
        i = rem(div(n, 2) + 2, Z)
        return div(i + 1, 2) * (2 * rem(i, 2) - 1)

    def at(self, z, e):
        return z * Y + self.g * 3 + e * (1 - 2 * self.g)

    def target_z(self, n):
        return lax.rem(self.z + self.offset(n) + Z, Z)

    def source_z(self, n):
        return lax.rem(self.z - self.offset(n) + Z, Z)

    def slot_there(self, n):
        return 2 * div(n, 2) + self.e


def all_slots(me, body):
    for n in range(16):
        if n in (12, 13):
            pl.when(n != me.own)(lambda n=n: body(n))
        else:
            body(n)


def loop(count, body):
    def step(n, carry):
        body(n)
        return carry

    lax.fori_loop(0, count, step, 0)


def scores_of(k, q):
    return lax.dot_general(k, q, (((1,), (0,)), ((), ())), preferred_element_type=f32)


def by_eight(x):
    return x.reshape(x.shape[0] // 8, 8, TQ)


def attention_step(q, top, scale, kk, vt, x_ref, y_ref, scores=True, exps=True):
    m = jnp.full((8, TQ), -jnp.inf, f32)
    total = jnp.zeros((8, TQ), f32)
    out = None
    tops = jnp.broadcast_to(top, (8, TQ)) if exps else None
    scales = jnp.broadcast_to(scale, (8, TQ))
    zeros = []
    for j in range(KEYS // KC):
        at = slice(j * KC, (j + 1) * KC)
        if exps:
            e = jnp.exp2(by_eight(y_ref[at, :]) - tops)
            y_ref[at, :] = e.reshape(KC, TQ)
            part = jnp.sum(e, axis=0)
            total = total + part
            zeros.append(jnp.minimum(part, 0.0))
        by = scales + zeros[j - 2] if exps and j >= 2 else scales
        weights = (by_eight(x_ref[at, :]) * by).reshape(KC, TQ).astype(bf16)
        part = lax.dot_general(vt[:, at], weights, (((1,), (0,)), ((), ())), preferred_element_type=f32)
        out = part if out is None else out + part
        if scores:
            s = scores_of(kk[at, :], q)
            x_ref[at, :] = s
            m = jnp.maximum(m, jnp.max(by_eight(s), axis=0))
    return m, total, out


def layer(
    q_ref, k_ref, v_ref, w_ref, qg_ref, kg_ref, out_ref,
    kvs, qs, kvr, qr, kk, vt, qt, s0, s1, ot, atts, attr, wf,
    kv_ss, kv_rs, fw_ss, fw_rs, q_ss, q_rs, at_ss, at_rs, w_ss, w_rs, own_sem,
    k_in, v_in, q_in, in_sem,
):
    me = Place()

    def remote(src, dst, ss, rs, **device):
        return pltpu.make_async_remote_copy(
            src_ref=src, dst_ref=dst, send_sem=ss, recv_sem=rs, device_id=device, device_id_type=MESH
        )

    barrier = pltpu.get_barrier_semaphore()

    def hello(**device):
        pl.semaphore_signal(barrier, inc=1, device_id=device, device_id_type=MESH)

    inputs = [
        pltpu.make_async_copy(src.at[0], dst, in_sem.at[n])
        for n, (src, dst) in enumerate(((k_ref, k_in), (v_ref, v_in), (q_ref, q_in)))
    ]
    for copy in inputs:
        copy.start()
    all_slots(me, lambda n: hello(sp=me.at(me.target_z(n), rem(n, 2))))
    hello(sp=me.partner)
    hello(dp=me.sib)
    hello(dp=me.left)
    hello(dp=me.right)

    tables = rotary_tables(lax.axis_index("sp") * TOK)
    ones = head_sums()

    def two_heads(ref):
        gain = ref[...].reshape(1, HD)
        return jnp.concatenate([gain, gain], axis=1)

    q_gain, k_gain = two_heads(qg_ref), two_heads(kg_ref)
    first_head = lanes(TOK) < HD

    def make_kv(i):
        at = pl.ds(pl.multiple_of(me.target_z(2 * i) * 2 * HD, 2 * HD), 2 * HD)
        k = turned(k_in[:, at].astype(f32), k_gain, tables, ones)
        v = v_in[:, at].astype(f32)
        kvs[2 * i] = jnp.where(first_head, k, pltpu.roll(v, HD, 1)).astype(bf16)
        kvs[2 * i + 1] = jnp.where(first_head, pltpu.roll(k, HD, 1), v).astype(bf16)

    def make_q(n):
        j = 2 * me.target_z(n) + rem(n, 2)
        at = pl.ds(pl.multiple_of(j * 2 * HD, 2 * HD), 2 * HD)
        qs[n] = turned(q_in[:, at].astype(f32), q_gain, tables, ones).astype(bf16)

    def kv_copy(n):
        there = me.slot_there(n)
        return remote(
            kvs.at[n], kvr.at[0, there], kv_ss.at[n], kv_rs.at[there],
            sp=me.at(me.target_z(n), rem(n, 2)),
        )

    def q_copy(n):
        there = me.slot_there(n)
        return remote(
            qs.at[n], qr.at[there], q_ss.at[n], q_rs.at[there],
            sp=me.at(me.target_z(n), rem(n, 2)),
        )

    def fw_copy(n):
        return remote(kvr.at[0, n], kvr.at[1, n], fw_ss.at[n], fw_rs.at[n], sp=me.partner)

    def at_copy(n):
        return remote(
            atts.at[n], attr.at[me.head], at_ss.at[n], at_rs.at[me.head],
            sp=me.at(me.source_z(n), rem(n, 2)),
        )

    def arrival(ref, ss, rs):
        return remote(ref, ref, ss, rs, sp=me.partner)

    top_half, low_half = pl.ds(0, W_ROWS // 2), pl.ds(W_ROWS // 2, W_ROWS // 2)

    def w_copy(kind, src, dst, dp):
        return remote(src, dst, w_ss.at[kind], w_rs.at[kind], dp=dp)

    w_own = (
        w_copy(0, w_ref, wf.at[me.dp], me.sib),
        w_copy(1, w_ref, wf.at[me.dp], me.right),
        w_copy(2, w_ref, wf.at[me.dp], me.left),
    )
    w_next = (
        w_copy(3, wf.at[me.left, top_half], wf.at[me.left, top_half], me.right),
        w_copy(4, wf.at[me.right, low_half], wf.at[me.right, low_half], me.left),
        w_copy(5, wf.at[me.left], wf.at[me.left], me.sib),
        w_copy(6, wf.at[me.right], wf.at[me.right], me.sib),
    )
    w_last = (
        w_copy(7, wf.at[me.opp, top_half], wf.at[me.opp, top_half], me.sib),
        w_copy(8, wf.at[me.opp, low_half], wf.at[me.opp, low_half], me.sib),
    )

    def w_arrival(kind, ref):
        arrival(ref, w_ss.at[kind], w_rs.at[kind]).wait_recv()

    def make_four(r):
        make_kv(2 * r)
        make_kv(2 * r + 1)

    inputs[0].wait()
    inputs[1].wait()
    loop(4, make_four)
    pl.semaphore_wait(barrier, 19)

    all_slots(me, lambda n: kv_copy(n).start())
    kvr[0, me.own] = kvs[me.own]

    def make_q_four(r):
        for n in range(4):
            make_q(4 * r + n)

    inputs[2].wait()
    loop(4, make_q_four)

    all_slots(me, lambda n: q_copy(n).start())
    qr[me.own] = qs[me.own]
    fw_copy(me.own).start()
    own_w = pltpu.make_async_copy(w_ref, wf.at[me.dp], own_sem)
    own_w.start()
    for copy in w_own:
        copy.start()

    def forward(n):
        @pl.when(n != me.own)
        def _():
            arrival(kvr.at[0, n], kv_ss.at[n], kv_rs.at[n]).wait_recv()
            fw_copy(n).start()


    def make_keys(half, g):
        block = kvr[half, pl.ds(GROUP * g, GROUP)].reshape(SPAN, 2 * HD)
        at = pl.ds(pl.multiple_of((half * GROUP + g) * SPAN, 128), SPAN)
        twice = jnp.concatenate([block[:, :HD], block[:, :HD]], axis=1)
        kk[at, :] = twice
        vt[:, at] = jnp.transpose(block)[HD:]

    def make_queries(g):
        def wait(r):
            n = GROUP * g + r

            @pl.when(n != me.own)
            def _():
                arrival(qr.at[n], q_ss.at[n], q_rs.at[n]).wait_recv()

        loop(4, wait)
        block = qr[pl.ds(GROUP * g, GROUP)].reshape(SPAN, 2 * HD)
        t = jnp.transpose(block.astype(f32)) * log2_scale
        t = jnp.concatenate([t[:HD], t[HD:]], axis=1)
        first = t.astype(bf16)
        second = (t - first.astype(f32)).astype(bf16)
        terms = jnp.concatenate([first, second], axis=0)
        for u in range(5):
            qt[5 * g + u] = terms[:, u * TQ : (u + 1) * TQ]

    def send_back(g):
        tiles = jnp.concatenate([ot[5 * g + u] for u in range(5)], axis=1)
        heads = jnp.concatenate([tiles[:, :SPAN], tiles[:, SPAN:]], axis=0)
        atts[pl.ds(GROUP * g, GROUP)] = jnp.transpose(heads).astype(bf16).reshape(GROUP, TOK, 2 * HD)

        def send(r):
            n = GROUP * g + r

            @pl.when(n != me.own)
            def _():
                at_copy(n).start()

        loop(4, send)

    row_top = lambda m: jnp.max(m, axis=0, keepdims=True)
    row_scale = lambda total: 1.0 / jnp.sum(total, axis=0, keepdims=True)
    s1[...] = jnp.zeros_like(s1)

    def own_keys(g):
        loop(GROUP, lambda r: forward(GROUP * g + r))
        make_keys(0, g)

    loop(4, own_keys)
    make_queries(0)

    def first_scores(half, g, m):
        at = pl.ds(pl.multiple_of((half * GROUP + g) * SPAN, 128), SPAN)
        s = scores_of(kk[at, :], qt[0])
        s0[at, :] = s
        return jnp.maximum(m, jnp.max(by_eight(s), axis=0))

    def partner_keys(g, m):
        def wait(n):
            arrival(kvr.at[1, GROUP * g + n], fw_ss.at[GROUP * g + n], fw_rs.at[GROUP * g + n]).wait_recv()

        loop(4, wait)
        make_keys(1, g)
        return first_scores(1, g, m)

    m = jnp.full((8, TQ), -jnp.inf, f32)
    m = lax.fori_loop(0, 4, lambda g, m: first_scores(0, g, m), m)
    m = lax.fori_loop(0, 4, partner_keys, m)

    def two_tiles(p, carry):
        top, scale = carry

        @pl.when(jnp.logical_or(p == 2, jnp.logical_or(p == 4, p == 7)))
        def _():
            make_queries(lax.div(p, 2))

        m, total, out = attention_step(qt[2 * p + 1], top, scale, kk, vt, s1, s0)
        ot[jnp.maximum(2 * p - 1, 0)] = out
        top, scale = row_top(m), row_scale(total)

        @pl.when(p == 3)
        def _():
            w_arrival(1, wf.at[me.left])
            w_arrival(2, wf.at[me.right])
            for copy in w_next:
                copy.start()

        @pl.when(p == 8)
        def _():
            w_arrival(3, wf.at[me.opp, top_half])
            w_arrival(4, wf.at[me.opp, low_half])
            for copy in w_last:
                copy.start()

        m, total, out = attention_step(
            qt[jnp.minimum(2 * p + 2, TILES - 1)], top, scale, kk, vt, s0, s1
        )
        ot[2 * p] = out

        @pl.when(jnp.logical_or(p == 2, jnp.logical_or(p == 5, p == 7)))
        def _():
            send_back(lax.div(p, 3))

        return row_top(m), row_scale(total)

    _, scale = lax.fori_loop(
        0, TILES // 2, two_tiles, (row_top(m), jnp.zeros((1, TQ), f32))
    )
    _, _, out = attention_step(None, None, scale, kk, vt, s1, None, scores=False, exps=False)
    ot[TILES - 1] = out
    send_back(3)
    attr[me.head] = atts[me.own]

    def sent(n):
        @pl.when(n != me.own)
        def _():
            kv_copy(n).wait_send()
            q_copy(n).wait_send()

        fw_copy(n).wait_send()

    loop(16, sent)
    loop(12, lambda n: at_copy(n).wait_send())
    for copy in w_own + w_next + w_last:
        copy.wait_send()

    w_arrival(0, wf.at[me.sib])
    other = me.sib - me.dp
    w_arrival(5, wf.at[me.left + other])
    w_arrival(6, wf.at[me.right + other])
    w_arrival(7, wf.at[me.opp + other, top_half])
    w_arrival(8, wf.at[me.opp + other, low_half])
    own_w.wait()

    def heads_in(j):
        @pl.when(j != me.head)
        def _():
            arrival(attr.at[j], at_ss.at[j], at_rs.at[j]).wait_recv()

    loop(16, heads_in)

    def project(n):
        rows = jnp.concatenate([attr[j] for j in range(KV)], axis=1)
        product = lax.dot_general(rows, wf[n], (((1,), (0,)), ((), ())), preferred_element_type=f32)
        out_ref[0, :, pl.ds(pl.multiple_of(n * W_COLS, W_COLS), W_COLS)] = product.astype(bf16)

    loop(8, project)

    for n in range(12, 16):
        if n < 14:
            pl.when(n != me.own)(lambda n=n: at_copy(n).wait_send())
        else:
            at_copy(n).wait_send()


def on_device(queries, keys, values, q_gain, k_gain, w_out):
    dma = pltpu.SemaphoreType.DMA
    vmem = pl.BlockSpec(memory_space=pltpu.VMEM)
    anywhere = pl.BlockSpec(memory_space=pl.ANY)
    return pl.pallas_call(
        layer,
        out_shape=jax.ShapeDtypeStruct((1, TOK, W_ROWS), bf16),
        in_specs=[anywhere] * 4 + [vmem] * 2,
        out_specs=vmem,
        scratch_shapes=[
            pltpu.VMEM((16, TOK, 128), bf16),
            pltpu.VMEM((16, TOK, 128), bf16),
            pltpu.VMEM((2, 16, TOK, 128), bf16),
            pltpu.VMEM((16, TOK, 128), bf16),
            pltpu.VMEM((KEYS, 128), bf16),
            pltpu.VMEM((HD, KEYS), bf16),
            pltpu.VMEM((TILES, 2 * HD, TQ), bf16),
            pltpu.VMEM((KEYS, TQ), f32),
            pltpu.VMEM((KEYS, TQ), f32),
            pltpu.VMEM((TILES, HD, TQ), f32),
            pltpu.VMEM((16, TOK, 128), bf16),
            pltpu.VMEM((16, TOK, 128), bf16),
            pltpu.VMEM((8, W_ROWS, W_COLS), bf16),
            dma((16,)), dma((16,)), dma((16,)), dma((16,)),
            dma((16,)), dma((16,)), dma((16,)), dma((16,)),
            dma((9,)), dma((9,)), dma,
            pltpu.VMEM((TOK, KV * HD), bf16),
            pltpu.VMEM((TOK, KV * HD), bf16),
            pltpu.VMEM((TOK, QH * HD), bf16),
            dma((3,)),
        ],
        compiler_params=pltpu.CompilerParams(
            collective_id=0, has_side_effects=True, vmem_limit_bytes=60 * 2**20
        ),
    )(
        jnp.swapaxes(queries, 1, 2),
        jnp.swapaxes(keys, 1, 2),
        jnp.swapaxes(values, 1, 2),
        w_out,
        q_gain,
        k_gain,
    )


def solution(mesh):
    return jax.shard_map(
        on_device,
        mesh=mesh,
        in_specs=(P("dp", None, "sp"), P("dp", None, "sp"), P("dp", None, "sp"), P(), P(), P(None, "dp")),
        out_specs=P("dp", "sp", None),
        check_vma=False,
    )
```
